256 devices in a mesh: sp: 64 (over z, y, core), tp: 4 (over x).
Axes of the slice: x: 4, y: 4, z: 8, core: 2. Of those that a mesh axis runs over, the one named last changes fastest.
Arguments:
- stream_in: bfloat16 [16384, 4096], P(('sp', 'tp')), may hold values from -6 to 6
- q_first: bfloat16 [16384, 1024], P('sp', 'tp'), may hold values from -110 to 110
- q_second: bfloat16 [16384, 1024], P('sp', 'tp'), may hold values from -110 to 110
- k_first: bfloat16 [16384, 512], P('sp', 'tp'), may hold values from -7 to 7
- k_second: bfloat16 [16384, 512], P('sp', 'tp'), may hold values from -7 to 7
- values: bfloat16 [16384, 1024], P('sp', 'tp'), may hold values from -6 to 6
- head_lambda: float32 [8], P('tp'), may hold values from 0.3 to 0.8
- w_out: bfloat16 [2048, 4096], P('tp'), may hold values from -0.125 to 0.125
- norm_gain: float32 [4096], replicated, may hold values from 0.1 to 1.9
- routes: int32 [16384, 4], P(('sp', 'tp')), may hold values from 0 to 63, all different within a row; in each aligned block of 64 rows (0 to 63, 64 to 127, ...) at most 6 rows name the same one
- route_w: float32 [16384, 4], P(('sp', 'tp')), may hold values from 0.2 to 1
- w_gate: bfloat16 [64, 4096, 128], P('sp'), may hold values from -0.09375 to 0.09375
- w_up: bfloat16 [64, 4096, 128], P('sp'), may hold values from -0.09375 to 0.09375
- w_down: bfloat16 [64, 128, 4096], P('sp'), may hold values from -0.5 to 0.5
- s_gate: bfloat16 [4096, 512], P(None, 'tp'), may hold values from -0.09375 to 0.09375
- s_up: bfloat16 [4096, 512], P(None, 'tp'), may hold values from -0.09375 to 0.09375
- s_down: bfloat16 [512, 4096], P('tp'), may hold values from -0.25 to 0.25
Outputs:
- layer_out: bfloat16 [16384, 4096], P(('sp', 'tp'))
The draws below stay inside these ranges and needn't reach their ends.
Inputs may be any that keep to these rules, and one draw needn't show every extreme that they name: `routes`: each row names 4 different experts. Within the rows of one device (aligned blocks of 64 rows) no expert is named more than 6 times, and in some blocks one expert is named exactly 6 times.
All inputs are finite; a program needn't handle non-finite values.
Results may differ from the reference program's by a relative error of at most 0.017.
Values may be sent and summed in bfloat16 or wider, within the bound.
A program may use at most 128 MiB of HBM per device.

```python
import math
import jax
import jax.numpy as jnp
import numpy as np
from jax import lax

D = 4096
HEAD = 128
HEADS = 8
KV_HEADS = 4
VD = 256
F = 128
SF = 512
TOPK = 4
ROWS = 64
TOKENS = 16384
EXP = 64
CAP = 6
N_SP = 64
N_TP = 4


def key_table(key, which):
    raw = jnp.clip(jax.random.normal(jax.random.fold_in(key, 100 + which), (TOKENS, KV_HEADS * HEAD), jnp.float32), -4.5, 4.5) * 1.3
    return raw


def query_table(key, which):
    raw = jnp.clip(jax.random.normal(jax.random.fold_in(key, 300 + which), (TOKENS, HEADS * HEAD), jnp.float32), -4.5, 4.5) * 1.3
    return raw


def draw_q_first(key, part):
    return query_table(key, 1).astype(jnp.bfloat16)


def draw_q_second(key, part):
    return query_table(key, 2).astype(jnp.bfloat16)


def draw_k_first(key, part):
    return key_table(key, 1).astype(jnp.bfloat16)


def draw_k_second(key, part):
    return key_table(key, 2).astype(jnp.bfloat16)


def level_of(rng, shape, split, smallest, largest):
    factor_of = 1.0
    for axis_at, blocks in split:
        draws = jax.random.uniform(jax.random.fold_in(jax.random.fold_in(rng, 6), axis_at), (blocks,), jnp.float32, smallest / len(split), largest / len(split))
        factor_of = factor_of * jnp.repeat(jnp.exp(draws), shape[axis_at] // blocks).reshape((-1,) + (1,) * (len(shape) - 1 - axis_at))
    return factor_of


def routed_block(own_key, own, number, rows, amount, top, bound, lean):
    ranking = jax.random.permutation(own_key, amount)
    packed, common = shares(amount, rows * top, bound, lean, True), shares(amount, rows * top, bound, lean, False)
    places = jnp.arange(amount)

    def named(tallies, rotation):
        used = int((tallies > 0).sum())
        fixed = max(1, used // 4)
        shifted = fixed + (places - fixed + rotation * (used - fixed)) % max(1, amount - fixed)
        return jnp.zeros((amount,), jnp.int32).at[ranking[jnp.where(places < fixed, places, shifted)]].set(jnp.asarray(tallies, jnp.int32))

    tallies = jnp.where(number % 4 == 0, named(packed, number // 4), named(common, number - number // 4 - 1))
    mixed = jax.random.permutation(jax.random.fold_in(own, 3), amount)
    source_of, sink = mixed[0:amount // 2 * 2:2], mixed[1:amount // 2 * 2:2]
    margin = jnp.minimum(tallies[source_of] - 1, bound - tallies[sink]) // 2
    margin = jnp.where((source_of == ranking[0]) | (sink == ranking[0]) | (tallies[sink] == 0), 0, jnp.maximum(margin, 0))
    shifted = jax.random.randint(jax.random.fold_in(own, 4), (amount // 2,), 0, 1 << 20) % (margin + 1)
    tallies = tallies.at[source_of].add(-shifted).at[sink].add(shifted)
    labels = jnp.searchsorted(jnp.cumsum(tallies), jnp.arange(rows * top), side="right").astype(jnp.int32)
    grid = labels.reshape(top, rows).T
    grid = grid[jax.random.permutation(jax.random.fold_in(own, 1), rows)]
    rotation = jax.random.randint(jax.random.fold_in(own, 2), (rows, 1), 0, top)
    return jnp.take_along_axis(grid, (jnp.arange(top)[None, :] + rotation) % top, axis=1)


def shares(amount, total, limit, skew, full):
    loads = [(1 << 20) // math.isqrt(standing ** skew) + 1 for standing in range(1, amount + 1)]
    largest = limit if full else min(limit, max(-(-total // amount), total * loads[0] // sum(loads)))
    least = 1 if total - largest >= amount - 1 else 0
    holding, spare = [largest] + [least] * (amount - 1), total - largest - least * (amount - 1)
    while spare > 0:
        candidates = [i for i in range(1, amount) if holding[i] < largest] or [i for i in range(1, amount) if holding[i] < limit]
        mass, left = sum([loads[i] for i in candidates]), spare
        for i in candidates:
            addition = min(limit - holding[i], max(1, left * loads[i] // mass), spare)
            holding[i] = holding[i] + addition
            spare = spare - addition
    return np.array(holding)


def normal_values(key, extent, deviation, most, shards=(), held_as=jnp.bfloat16):
    loudness = level_of(key, extent, shards, -0.22, 0.18) if shards else 1.0
    drawn = jax.random.normal(key, extent, jnp.float32) * deviation * loudness
    return jnp.minimum(jnp.maximum(drawn, -most), most).astype(held_as)


def setup_inputs(seed: int = 0) -> dict:
    keys = jax.random.split(jax.random.key(seed), 18)
    stream_in = normal_values(keys[0], (TOKENS, D), 1.0, 6.0, ((0, 256),))
    q_first = draw_q_first(jax.random.fold_in(keys[17], 71), 0)
    q_second = draw_q_second(jax.random.fold_in(keys[17], 71), 0)
    k_first = draw_k_first(jax.random.fold_in(keys[17], 71), 0)
    k_second = draw_k_second(jax.random.fold_in(keys[17], 71), 0)
    values = normal_values(keys[5], (TOKENS, KV_HEADS * VD), 1.0, 6.0, ((0, 64), (1, 4)))
    head_lambda = jnp.clip(0.3 + 0.5 * jax.random.uniform(keys[6], (HEADS,), jnp.float32) ** level_of(keys[6], (HEADS,), ((0, 4),), -0.2, 0.2), 0.3, 0.8)
    w_out = normal_values(keys[7], (HEADS * VD, D), (HEADS * VD) ** -0.5, 0.125, ((0, 4),))
    norm_gain = jnp.clip(1.0 + 0.18 * jax.random.normal(keys[8], (D,), jnp.float32), 0.1, 1.9)
    routes_keys = jax.random.split(jax.random.fold_in(keys[9], 1), TOKENS // ROWS)
    routes_turns = jax.random.permutation(jax.random.fold_in(keys[9], 3), TOKENS // ROWS)
    routes = jax.vmap(lambda own, number: routed_block(jax.random.fold_in(keys[9], 2), own, number, ROWS, EXP, TOPK, CAP, 1))(routes_keys, routes_turns).reshape((TOKENS, TOPK))
    route_w = jnp.clip(0.2 + 0.8 * jax.random.uniform(keys[10], (TOKENS, TOPK), jnp.float32) ** level_of(keys[10], (TOKENS, TOPK), ((0, 256),), -0.2, 0.2), 0.2, 1.0)
    w_gate = normal_values(keys[11], (EXP, D, F), D ** -0.5, 0.09375, ((0, 64),))
    w_up = normal_values(keys[12], (EXP, D, F), D ** -0.5, 0.09375, ((0, 64),))
    w_down = normal_values(keys[13], (EXP, F, D), F ** -0.5, 0.5, ((0, 64),))
    s_gate = normal_values(keys[14], (D, SF), D ** -0.5, 0.09375, ((1, 4),))
    s_up = normal_values(keys[15], (D, SF), D ** -0.5, 0.09375, ((1, 4),))
    s_down = normal_values(keys[16], (SF, D), SF ** -0.5, 0.25, ((0, 4),))
    return {"stream_in": stream_in, "q_first": q_first, "q_second": q_second, "k_first": k_first, "k_second": k_second, "values": values, "head_lambda": head_lambda, "w_out": w_out, "norm_gain": norm_gain, "routes": routes, "route_w": route_w, "w_gate": w_gate, "w_up": w_up, "w_down": w_down, "s_gate": s_gate, "s_up": s_up, "s_down": s_down}


FLOOR = -1e+30

def absorb(state, first_q, second_q, first_k, second_k, value_rows, query_pos, key_pos):
    allowed = key_pos[None, :] <= query_pos[:, None]
    scale = first_q.shape[-1] ** (-0.5)
    result = []
    pairs = ((first_q, first_k), (second_q, second_k))
    for index in range(2):
        query_rows, key_rows = pairs[index]
        peak, total, accum = (state[3 * index], state[3 * index + 1], state[3 * index + 2])
        scores = jnp.dot(query_rows, key_rows.T, preferred_element_type=jnp.float32) * scale
        scores = jnp.where(allowed, scores, FLOOR)
        raised = jnp.maximum(peak, scores.max(-1))
        weights = jnp.where(allowed, jnp.exp(scores - raised[:, None]), 0.0)
        fade = jnp.exp(peak - raised)
        total = total * fade + weights.sum(-1)
        accum = accum * fade[:, None] + jnp.dot(weights.astype(jnp.bfloat16), value_rows, preferred_element_type=jnp.float32)
        result += [raised, total, accum]
    return tuple(result)

def one_head(first_q, second_q, first_k, second_k, value_rows, weight, span, blocks):

    def per_block(block):
        begin = block * span
        query_one = lax.dynamic_slice_in_dim(first_q, begin, span, 0)
        query_two = lax.dynamic_slice_in_dim(second_q, begin, span, 0)
        query_pos = begin + jnp.arange(span, dtype=jnp.int32)
        peaks = jnp.full((span,), FLOOR, jnp.float32)
        sums = jnp.zeros((span,), jnp.float32)
        accums = jnp.zeros((span, VD), jnp.float32)
        start_state = (peaks, sums, accums, peaks, sums, accums)

        def visit(inner, state):
            key_begin = inner * span
            key_one = lax.dynamic_slice_in_dim(first_k, key_begin, span, 0)
            key_two = lax.dynamic_slice_in_dim(second_k, key_begin, span, 0)
            value_part = lax.dynamic_slice_in_dim(value_rows, key_begin, span, 0)
            key_pos = key_begin + jnp.arange(span, dtype=jnp.int32)
            return absorb(state, query_one, query_two, key_one, key_two, value_part, query_pos, key_pos)
        final = lax.fori_loop(jnp.int32(0), block + 1, visit, start_state)
        head_out = final[2] / final[1][:, None] - weight * final[5] / final[4][:, None]
        head_out = head_out * lax.rsqrt(lax.optimization_barrier(jnp.mean(head_out * head_out, axis=-1, keepdims=True)) + 1e-05)
        return head_out.astype(jnp.bfloat16)
    outputs = lax.map(per_block, jnp.arange(blocks, dtype=jnp.int32))
    return outputs.reshape(TOKENS, VD)

def reference(stream_in, q_first, q_second, k_first, k_second, values, head_lambda, w_out, norm_gain, routes, route_w, w_gate, w_up, w_down, s_gate, s_up, s_down):
    group = HEADS // KV_HEADS
    span = math.gcd(TOKENS, 512)
    blocks = TOKENS // span
    parts = []
    for head in range(HEADS):
        key_head = head // group
        parts.append(one_head(q_first[:, head * HEAD:(head + 1) * HEAD], q_second[:, head * HEAD:(head + 1) * HEAD], k_first[:, key_head * HEAD:(key_head + 1) * HEAD], k_second[:, key_head * HEAD:(key_head + 1) * HEAD], values[:, key_head * VD:(key_head + 1) * VD], head_lambda[head], span, blocks))
    attn_rows = jnp.concatenate(parts, axis=1)
    attn = jnp.dot(attn_rows, w_out, preferred_element_type=jnp.float32)
    resid = (stream_in.astype(jnp.float32) + attn).astype(jnp.bfloat16)
    stream = lax.optimization_barrier(resid).astype(jnp.float32)
    normed = (stream * lax.rsqrt(lax.optimization_barrier(jnp.mean(stream * stream, axis=-1, keepdims=True)) + 1e-06) * norm_gain).astype(jnp.bfloat16)
    shared_hidden = (jax.nn.silu(jnp.dot(normed, s_gate, preferred_element_type=jnp.float32)) * jnp.dot(normed, s_up, preferred_element_type=jnp.float32)).astype(jnp.bfloat16)
    shared = jnp.dot(shared_hidden, s_down, preferred_element_type=jnp.float32)
    flat_ids = routes.reshape(-1).astype(jnp.int32)
    count_all = TOKENS * TOPK
    token_of = jnp.arange(count_all, dtype=jnp.int32) // TOPK
    order = jnp.argsort(flat_ids, stable=True).astype(jnp.int32)
    counts = lax.optimization_barrier(jnp.sum((flat_ids[None, :] == jnp.arange(EXP, dtype=jnp.int32)[:, None]).astype(jnp.int32), axis=1)).astype(jnp.int32)
    starts = (jnp.cumsum(counts) - counts).astype(jnp.int32)
    window = N_SP * N_TP * CAP
    padded = jnp.concatenate([order, jnp.zeros((window,), jnp.int32)])
    flat_weights = route_w.reshape(-1)

    def serve(routed, inputs):
        gate_e, up_e, down_e, begin, count = inputs
        picks = lax.dynamic_slice_in_dim(padded, begin, window, 0)
        live = jnp.arange(window, dtype=jnp.int32) < count
        tokens_here = token_of[picks]
        rows_here = normed[tokens_here]
        hidden = (jax.nn.silu(jnp.dot(rows_here, gate_e, preferred_element_type=jnp.float32)) * jnp.dot(rows_here, up_e, preferred_element_type=jnp.float32)).astype(jnp.bfloat16)
        result = jnp.dot(hidden, down_e, preferred_element_type=jnp.float32).astype(jnp.bfloat16)
        scaled = result.astype(jnp.float32) * jnp.where(live, flat_weights[picks], 0.0)[:, None]
        return (routed.at[tokens_here].add(scaled), None)
    routed, _ = lax.scan(serve, jnp.zeros((TOKENS, D), jnp.float32), (w_gate, w_up, w_down, starts, counts))
    return (stream + routed + shared).astype(jnp.bfloat16)
```

```python
import functools
import math

import jax
import jax.numpy as jnp
from jax import lax
from jax.experimental import pallas as pl
from jax.experimental.pallas import tpu as pltpu
from jax.sharding import PartitionSpec as P

HEAD = 128
VD = 256
FLOOR = -1e30
NZ = 8
NY = 4
NCHIP = NZ * NY
BLK = 256
PAIR = 2 * BLK
KVW = 512
LOG2E = 1.4426950408889634

ORDER = sorted(
    [(dz, dy) for dz in (0, 1, -1, 2, -2, 3, -3, 4) for dy in (0, 1, -1, 2)],
    key=lambda a: (abs(a[0]) + abs(a[1]), -abs(a[0]), a),
)
PIECES = ((0, 80, "z", 1), (80, 80, "z", -1), (160, 48, "y", 1), (208, 48, "y", -1))


def step_counts():
    sent = {"z+": 0, "z-": 0, "y+": 0, "y-": 0}
    for dz, dy in ORDER:
        for _, rows, first, way in PIECES:
            for link, go in hops(dz, dy, first, way).items():
                if go:
                    sent[link] += rows
    return sent


def hops(dz, dy, first, way):
    zup = (dz >= 0) & (dz < (4 if way > 0 else 3))
    zdown = (dz <= 0) & (dz > (-3 if way > 0 else -4))
    yup = (dy >= 0) & (dy < (2 if way > 0 else 1))
    ydown = (dy <= 0) & (dy > (-1 if way > 0 else -2))
    if first == "z":
        zup, zdown = zup & (dy == 0), zdown & (dy == 0)
    else:
        yup, ydown = yup & (dz == 0), ydown & (dz == 0)
    return {"z+": zup, "z-": zdown, "y+": yup, "y-": ydown}


def lookup(values, index):
    out = jnp.int32(values[0])
    for k, v in enumerate(values[1:], 1):
        out = jnp.where(index == k, jnp.int32(v), out)
    return out


def attn_kernel(
    lam_ref, q1_ref, q2_ref, k1_hbm, k2_hbm, v_hbm, out_ref,
    kv, q_s, m_s, l_s, acc_s, load_sem, send_sem, recv_sem, pair_sem,
):
    me = lax.axis_index("sp")
    c = me % 2
    y = (me // 2) % NY
    z = me // (2 * NY)
    chip = z * NY + y

    def at(zz, yy, cc):
        return {"sp": ((zz + NZ) % NZ) * (2 * NY) + ((yy + NY) % NY) * 2 + cc}

    peers = {
        "z+": at(z + 1, y, c), "z-": at(z - 1, y, c),
        "y+": at(z, y + 1, c), "y-": at(z, y - 1, c),
        "pair": at(z, y, 1 - c),
    }
    links = ("z+", "z-", "y+", "y-", "pair")

    own = pl.multiple_of(chip * PAIR + c * BLK, BLK)
    loads = []
    for k, (src, lo, hi) in enumerate(((k1_hbm, 0, 128), (k2_hbm, 128, 256), (v_hbm, 256, 512))):
        loads.append(pltpu.make_async_copy(src, kv.at[pl.ds(own, BLK), lo:hi], load_sem.at[k]))
        loads[-1].start()

    barrier = pltpu.get_barrier_semaphore()
    for link in links:
        pl.semaphore_signal(barrier, inc=1, device_id=peers[link], device_id_type=pl.DeviceIdType.MESH)

    scale = HEAD ** (-0.5) * LOG2E
    for k, ref in enumerate((q1_ref, q2_ref)):
        for h in range(2):
            q_s[k, h * BLK : (h + 1) * BLK, :] = ref[:, h * HEAD : (h + 1) * HEAD]
    m_s[...] = jnp.full_like(m_s, FLOOR)
    l_s[...] = jnp.zeros_like(l_s)
    acc_s[...] = jnp.zeros_like(acc_s)

    pl.semaphore_wait(barrier, len(links))
    for copy in loads:
        copy.wait()

    def rows_of(src_chip, core, first, rows):
        return kv.at[pl.ds(pl.multiple_of(src_chip * PAIR + core * BLK + first, 16), rows), :]

    def remote(ref, link, sem):
        return pltpu.make_async_remote_copy(
            src_ref=ref, dst_ref=ref, send_sem=send_sem.at[links.index(link)], recv_sem=sem,
            device_id=peers[link], device_id_type=pl.DeviceIdType.MESH,
        )

    def forward(dz, dy, src_chip):
        for first_row, rows, first, way in PIECES:
            for link, go in hops(dz, dy, first, way).items():

                @pl.when(go)
                def _():
                    remote(rows_of(src_chip, c, first_row, rows), link, recv_sem.at[src_chip]).start()

        remote(rows_of(src_chip, c, 0, BLK), "pair", pair_sem.at[src_chip]).start()

    def attend(src_chip, masked):
        base = pl.multiple_of(src_chip * PAIR, PAIR)
        value = kv[pl.ds(base, PAIR), 256:512]
        for k in range(2):
            key = kv[pl.ds(base, PAIR), k * HEAD : (k + 1) * HEAD]
            scores = lax.dot_general(
                q_s[k], key, (((1,), (1,)), ((), ())), preferred_element_type=jnp.float32
            ) * scale
            if masked:
                q_pos = lax.broadcasted_iota(jnp.int32, scores.shape, 0) % BLK + c * BLK
                k_pos = lax.broadcasted_iota(jnp.int32, scores.shape, 1)
                scores = jnp.where(k_pos <= q_pos, scores, FLOOR)
            old = m_s[k]
            new = jnp.maximum(old, jnp.max(scores, axis=1, keepdims=True))
            fade = jnp.exp2(old - new)
            weights = jnp.exp2(scores - jnp.tile(new, (1, PAIR // 128)))
            if masked:
                weights = jnp.where(k_pos <= q_pos, weights, 0.0)
            part = weights[:, 0:128]
            for t in range(1, PAIR // 128):
                part = part + weights[:, t * 128 : (t + 1) * 128]
            m_s[k] = new
            l_s[k] = l_s[k] * fade + part
            acc_s[k] = acc_s[k] * jnp.tile(fade, (1, VD // 128)) + jnp.dot(
                weights.astype(jnp.bfloat16), value, preferred_element_type=jnp.float32
            )

    forward(jnp.int32(0), jnp.int32(0), chip)

    dz_table = [o[0] for o in ORDER]
    dy_table = [o[1] for o in ORDER]

    def place(e):
        dz, dy = lookup(dz_table, e), lookup(dy_table, e)
        return dz, dy, ((z - dz + NZ) % NZ) * NY + (y - dy + NY) % NY

    def step(e, carry):
        @pl.when(e < NCHIP)
        def _():
            dz, dy, src = place(e)
            remote(rows_of(src, c, 0, BLK), "z+", recv_sem.at[src]).wait_recv()
            forward(dz, dy, src)

        _, _, last = place(e - 1)
        remote(rows_of(last, 1 - c, 0, BLK), "pair", pair_sem.at[last]).wait_recv()

        @pl.when(e == 1)
        def _():
            attend(chip, True)

        @pl.when((e > 1) & (last < chip))
        def _():
            attend(last, False)

        return carry

    lax.fori_loop(1, NCHIP + 1, step, 0)

    head_rows = []
    for k in range(2):
        total = jnp.sum(l_s[k], axis=1, keepdims=True)
        head_rows.append(acc_s[k] / total)
    for h in range(2):
        span = slice(h * BLK, (h + 1) * BLK)
        head = head_rows[0][span] - lam_ref[h] * head_rows[1][span]
        head = head * lax.rsqrt(jnp.mean(head * head, axis=1, keepdims=True) + 1e-05)
        out_ref[:, h * VD : (h + 1) * VD] = head.astype(jnp.bfloat16)

    for link, rows in step_counts().items():
        remote(kv.at[pl.ds(0, rows), :], link, recv_sem.at[0]).wait_send()
    remote(kv.at[pl.ds(0, NCHIP * BLK), :], "pair", recv_sem.at[0]).wait_send()


def attention(head_lambda, q_first, q_second, k_first, k_second, values):
    vmem = pl.BlockSpec(memory_space=pltpu.VMEM)
    hbm = pl.BlockSpec(memory_space=pl.ANY)
    return pl.pallas_call(
        attn_kernel,
        out_shape=jax.ShapeDtypeStruct((BLK, 2 * VD), jnp.bfloat16),
        in_specs=[pl.BlockSpec(memory_space=pltpu.SMEM), vmem, vmem, hbm, hbm, hbm],
        out_specs=vmem,
        scratch_shapes=[
            pltpu.VMEM((NCHIP * PAIR, KVW), jnp.bfloat16),
            pltpu.VMEM((2, 2 * BLK, HEAD), jnp.bfloat16),
            pltpu.VMEM((2, 2 * BLK, 128), jnp.float32),
            pltpu.VMEM((2, 2 * BLK, 128), jnp.float32),
            pltpu.VMEM((2, 2 * BLK, VD), jnp.float32),
            pltpu.SemaphoreType.DMA((3,)),
            pltpu.SemaphoreType.DMA((5,)),
            pltpu.SemaphoreType.DMA((NCHIP,)),
            pltpu.SemaphoreType.DMA((NCHIP,)),
        ],
        compiler_params=pltpu.CompilerParams(
            collective_id=0, has_side_effects=True, vmem_limit_bytes=48 * 1024 * 1024
        ),
        name="attend",
    )(head_lambda, q_first, q_second, k_first, k_second, values)


def cut_along(x, dim, count):
    shape = x.shape
    pieces = x.reshape(*shape[:dim], count, shape[dim] // count, *shape[dim + 1 :])
    return jnp.moveaxis(pieces, dim, 0)


def sum_at_owner(x, axis, dim):
    count = lax.axis_size(axis)
    pieces = lax.all_to_all(cut_along(x, dim, count), axis, 0, 0, tiled=True)
    return jnp.sum(pieces.astype(jnp.float32), axis=0)


def shared_part(normed, s_gate, s_up, s_down):
    piece = lax.all_gather(normed, "tp", axis=0, tiled=True)
    gate_part = jnp.dot(piece, s_gate, preferred_element_type=jnp.float32)
    up_part = jnp.dot(piece, s_up, preferred_element_type=jnp.float32)
    hidden = (jax.nn.silu(gate_part) * up_part).astype(jnp.bfloat16)
    terms = jnp.dot(hidden, s_down, preferred_element_type=jnp.float32)
    return lax.psum_scatter(
        terms.astype(jnp.bfloat16), "tp", scatter_dimension=0, tiled=True
    ).astype(jnp.float32)


def routed_part(normed, routes, route_w, w_gate, w_up, w_down):
    rows, topk = routes.shape
    local_experts = w_gate.shape[0]
    experts = local_experts * lax.axis_size("sp")
    slots = max(2, 3 * rows * topk // (2 * experts))
    flat_ids = routes.reshape(-1)
    hits = (flat_ids[:, None] == jnp.arange(experts, dtype=jnp.int32)[None, :]).astype(jnp.int32)
    slot_of = jnp.sum(jnp.cumsum(hits, axis=0) * hits, axis=1) - 1
    target = flat_ids * slots + slot_of
    placing = jnp.any(
        jnp.arange(experts * slots, dtype=jnp.int32)[:, None, None]
        == target.reshape(rows, topk)[None, :, :],
        axis=-1,
    ).astype(jnp.bfloat16)
    outgoing = (
        jnp.dot(placing, normed, preferred_element_type=jnp.float32)
        .astype(jnp.bfloat16)
        .reshape(experts, slots, normed.shape[1])
    )
    arrived = lax.all_to_all(outgoing, "sp", split_axis=0, concat_axis=0, tiled=True)
    sources = arrived.shape[0] // local_experts
    grouped = arrived.reshape(sources, local_experts, arrived.shape[1], arrived.shape[2])
    gate_part = jnp.einsum("sjcd,jdf->sjcf", grouped, w_gate, preferred_element_type=jnp.float32)
    up_part = jnp.einsum("sjcd,jdf->sjcf", grouped, w_up, preferred_element_type=jnp.float32)
    hidden = (jax.nn.silu(gate_part) * up_part).astype(jnp.bfloat16)
    result = jnp.einsum(
        "sjcf,jfd->sjcd", hidden, w_down, preferred_element_type=jnp.float32
    ).astype(jnp.bfloat16)
    returned = lax.all_to_all(
        result.reshape(arrived.shape), "sp", split_axis=0, concat_axis=0, tiled=True
    )
    picked = (
        returned.reshape(experts * slots, normed.shape[1])[target]
        .reshape(rows, topk, normed.shape[1])
        .astype(jnp.float32)
    )
    return jnp.sum(picked * route_w[..., None], axis=1)


def local(
    stream_in,
    q_first,
    q_second,
    k_first,
    k_second,
    values,
    head_lambda,
    w_out,
    norm_gain,
    routes,
    route_w,
    w_gate,
    w_up,
    w_down,
    s_gate,
    s_up,
    s_down,
):
    attn_rows = attention(head_lambda, q_first, q_second, k_first, k_second, values)
    attn = sum_at_owner(
        jnp.dot(attn_rows, w_out, preferred_element_type=jnp.float32).astype(jnp.bfloat16), "tp", 0
    )
    resid = (stream_in.astype(jnp.float32) + attn).astype(jnp.bfloat16)
    stream = lax.optimization_barrier(resid).astype(jnp.float32)
    normed = (
        stream * lax.rsqrt(jnp.mean(stream * stream, axis=-1, keepdims=True) + 1e-06) * norm_gain
    ).astype(jnp.bfloat16)
    routed = routed_part(normed, routes, route_w, w_gate, w_up, w_down)
    shared = shared_part(normed, s_gate, s_up, s_down)
    return (stream + routed + shared).astype(jnp.bfloat16)


def solution(mesh):
    return jax.shard_map(
        local,
        mesh=mesh,
        in_specs=(
            P(("sp", "tp"), None),
            P("sp", "tp"),
            P("sp", "tp"),
            P("sp", "tp"),
            P("sp", "tp"),
            P("sp", "tp"),
            P("tp"),
            P("tp", None),
            P(),
            P(("sp", "tp"), None),
            P(("sp", "tp"), None),
            P("sp", None, None),
            P("sp", None, None),
            P("sp", None, None),
            P(None, "tp"),
            P(None, "tp"),
            P("tp", None),
        ),
        out_specs=P(("sp", "tp"), None),
        check_vma=False,
    )
```

```python
import jax
import jax.numpy as jnp
from jax import lax
from jax.experimental import pallas as pl
from jax.experimental.pallas import tpu as pltpu
from jax.sharding import PartitionSpec as P

HEAD = 128
VD = 256
FLOOR = -1e30
NZ = 8
NY = 4
NCHIP = NZ * NY
BLK = 256
PAIR = 2 * BLK
KVW = 512
LOG2E = 1.4426950408889634

ORDER = sorted(
    [(dz, dy) for dz in (0, 1, -1, 2, -2, 3, -3, 4) for dy in (0, 1, -1, 2)],
    key=lambda a: (abs(a[0]) + abs(a[1]), -abs(a[0]), a),
)
PIECES = ((0, 80, "z", 1), (80, 80, "z", -1), (160, 48, "y", 1), (208, 48, "y", -1))


def step_counts():
    sent = {"z+": 0, "z-": 0, "y+": 0, "y-": 0}
    for dz, dy in ORDER:
        for _, rows, first, way in PIECES:
            for link, go in hops(dz, dy, first, way).items():
                if go:
                    sent[link] += rows
    return sent


def hops(dz, dy, first, way):
    zup = (dz >= 0) & (dz < (4 if way > 0 else 3))
    zdown = (dz <= 0) & (dz > (-3 if way > 0 else -4))
    yup = (dy >= 0) & (dy < (2 if way > 0 else 1))
    ydown = (dy <= 0) & (dy > (-1 if way > 0 else -2))
    if first == "z":
        zup, zdown = zup & (dy == 0), zdown & (dy == 0)
    else:
        yup, ydown = yup & (dz == 0), ydown & (dz == 0)
    return {"z+": zup, "z-": zdown, "y+": yup, "y-": ydown}


def lookup(values, index):
    out = jnp.int32(values[0])
    for k, v in enumerate(values[1:], 1):
        out = jnp.where(index == k, jnp.int32(v), out)
    return out


def attn_kernel(
    lam_ref, q1_ref, q2_ref, k1_hbm, k2_hbm, v_hbm, out_ref,
    kv, q_s, m_s, l_s, acc_s, load_sem, send_sem, recv_sem, pair_sem,
):
    me = lax.axis_index("sp")
    c = me % 2
    y = (me // 2) % NY
    z = me // (2 * NY)
    chip = z * NY + y

    def at(zz, yy, cc):
        return {"sp": ((zz + NZ) % NZ) * (2 * NY) + ((yy + NY) % NY) * 2 + cc}

    peers = {
        "z+": at(z + 1, y, c), "z-": at(z - 1, y, c),
        "y+": at(z, y + 1, c), "y-": at(z, y - 1, c),
        "pair": at(z, y, 1 - c),
    }
    links = ("z+", "z-", "y+", "y-", "pair")

    own = pl.multiple_of(chip * PAIR + c * BLK, BLK)
    loads = []
    for k, (src, lo, hi) in enumerate(((k1_hbm, 0, 128), (k2_hbm, 128, 256), (v_hbm, 256, 512))):
        loads.append(pltpu.make_async_copy(src, kv.at[pl.ds(own, BLK), lo:hi], load_sem.at[k]))
        loads[-1].start()

    barrier = pltpu.get_barrier_semaphore()
    for link in links:
        pl.semaphore_signal(barrier, inc=1, device_id=peers[link], device_id_type=pl.DeviceIdType.MESH)

    scale = HEAD ** (-0.5) * LOG2E
    for k, ref in enumerate((q1_ref, q2_ref)):
        for h in range(2):
            q_s[k, h * BLK : (h + 1) * BLK, :] = ref[:, h * HEAD : (h + 1) * HEAD]
    m_s[...] = jnp.full_like(m_s, FLOOR)
    l_s[...] = jnp.zeros_like(l_s)
    acc_s[...] = jnp.zeros_like(acc_s)

    pl.semaphore_wait(barrier, len(links))
    for copy in loads:
        copy.wait()

    def rows_of(src_chip, core, first, rows):
        return kv.at[pl.ds(pl.multiple_of(src_chip * PAIR + core * BLK + first, 16), rows), :]

    def remote(ref, link, sem):
        return pltpu.make_async_remote_copy(
            src_ref=ref, dst_ref=ref, send_sem=send_sem.at[links.index(link)], recv_sem=sem,
            device_id=peers[link], device_id_type=pl.DeviceIdType.MESH,
        )

    def forward(dz, dy, src_chip):
        for first_row, rows, first, way in PIECES:
            for link, go in hops(dz, dy, first, way).items():

                @pl.when(go)
                def _():
                    remote(rows_of(src_chip, c, first_row, rows), link, recv_sem.at[src_chip]).start()

        remote(rows_of(src_chip, c, 0, BLK), "pair", pair_sem.at[src_chip]).start()

    def attend(src_chip, masked):
        base = pl.multiple_of(src_chip * PAIR, PAIR)
        value = kv[pl.ds(base, PAIR), 256:512]
        for k in range(2):
            key = kv[pl.ds(base, PAIR), k * HEAD : (k + 1) * HEAD]
            scores = lax.dot_general(
                q_s[k], key, (((1,), (1,)), ((), ())), preferred_element_type=jnp.float32
            ) * scale
            if masked:
                q_pos = lax.broadcasted_iota(jnp.int32, scores.shape, 0) % BLK + c * BLK
                k_pos = lax.broadcasted_iota(jnp.int32, scores.shape, 1)
                scores = jnp.where(k_pos <= q_pos, scores, FLOOR)
            old = m_s[k]
            new = jnp.maximum(old, jnp.max(scores, axis=1, keepdims=True))
            fade = jnp.exp2(old - new)
            weights = jnp.exp2(scores - jnp.tile(new, (1, PAIR // 128)))
            if masked:
                weights = jnp.where(k_pos <= q_pos, weights, 0.0)
            part = weights[:, 0:128]
            for t in range(1, PAIR // 128):
                part = part + weights[:, t * 128 : (t + 1) * 128]
            m_s[k] = new
            l_s[k] = l_s[k] * fade + part
            acc_s[k] = acc_s[k] * jnp.tile(fade, (1, VD // 128)) + jnp.dot(
                weights.astype(jnp.bfloat16), value, preferred_element_type=jnp.float32
            )

    forward(jnp.int32(0), jnp.int32(0), chip)

    dz_table = [o[0] for o in ORDER]
    dy_table = [o[1] for o in ORDER]

    def place(e):
        dz, dy = lookup(dz_table, e), lookup(dy_table, e)
        return dz, dy, ((z - dz + NZ) % NZ) * NY + (y - dy + NY) % NY

    def step(e, carry):
        @pl.when(e < NCHIP)
        def _():
            dz, dy, src = place(e)
            remote(rows_of(src, c, 0, BLK), "z+", recv_sem.at[src]).wait_recv()
            forward(dz, dy, src)

        _, _, last = place(e - 1)
        remote(rows_of(last, 1 - c, 0, BLK), "pair", pair_sem.at[last]).wait_recv()

        @pl.when(e == 1)
        def _():
            attend(chip, True)

        @pl.when((e > 1) & (last < chip))
        def _():
            attend(last, False)

        return carry

    lax.fori_loop(1, NCHIP + 1, step, 0)

    head_rows = []
    for k in range(2):
        total = jnp.sum(l_s[k], axis=1, keepdims=True)
        head_rows.append(acc_s[k] / total)
    for h in range(2):
        span = slice(h * BLK, (h + 1) * BLK)
        head = head_rows[0][span] - lam_ref[h] * head_rows[1][span]
        head = head * lax.rsqrt(jnp.mean(head * head, axis=1, keepdims=True) + 1e-05)
        out_ref[:, h * VD : (h + 1) * VD] = head.astype(jnp.bfloat16)

    for link, rows in step_counts().items():
        remote(kv.at[pl.ds(0, rows), :], link, recv_sem.at[0]).wait_send()
    remote(kv.at[pl.ds(0, NCHIP * BLK), :], "pair", recv_sem.at[0]).wait_send()


def attention(head_lambda, q_first, q_second, k_first, k_second, values):
    vmem = pl.BlockSpec(memory_space=pltpu.VMEM)
    hbm = pl.BlockSpec(memory_space=pl.ANY)
    return pl.pallas_call(
        attn_kernel,
        out_shape=jax.ShapeDtypeStruct((BLK, 2 * VD), jnp.bfloat16),
        in_specs=[pl.BlockSpec(memory_space=pltpu.SMEM), vmem, vmem, hbm, hbm, hbm],
        out_specs=vmem,
        scratch_shapes=[
            pltpu.VMEM((NCHIP * PAIR, KVW), jnp.bfloat16),
            pltpu.VMEM((2, 2 * BLK, HEAD), jnp.bfloat16),
            pltpu.VMEM((2, 2 * BLK, 128), jnp.float32),
            pltpu.VMEM((2, 2 * BLK, 128), jnp.float32),
            pltpu.VMEM((2, 2 * BLK, VD), jnp.float32),
            pltpu.SemaphoreType.DMA((3,)),
            pltpu.SemaphoreType.DMA((5,)),
            pltpu.SemaphoreType.DMA((NCHIP,)),
            pltpu.SemaphoreType.DMA((NCHIP,)),
        ],
        compiler_params=pltpu.CompilerParams(
            collective_id=0, has_side_effects=True, vmem_limit_bytes=48 * 1024 * 1024
        ),
        name="attend",
    )(head_lambda, q_first, q_second, k_first, k_second, values)


D = 4096
ROWS = 64
TP = 4
SLAB = 2 * NY
CAP = 6
GROUP = NZ * CAP
SLOTS = SLAB * GROUP
NC = 8
W = D // NC
F = 128
MESH = pl.DeviceIdType.MESH
DISPATCH_LAGS = (1, 2, 3, 4, 5)
RETURN_LAGS = (1, 2, 4, 7, 9)


def moe_kernel(
    attn_ref, stream_ref, gain_ref, codes_ref,
    w_out_hbm, wg_hbm, wu_hbm, wd_hbm, sg_hbm, su_hbm, sd_hbm,
    out_ref,
    wo, wgu, wd, sgu, sd,
    op_all, op_in, resid_s, zbuf, cbuf, place_s, back_hi, back_lo,
    ysend, xbuf, hid_s, hb_s, rsend, ret, part_s, rs_out, rs_in,
    sh_all, sh_out, sh_in,
    wo_sem, load_sem, send_sem, op_sem, z_sem, code_sem, y_sem, r_sem, rs_sem, sh_sem, shr_sem,
):
    me = lax.axis_index("sp")
    tp = lax.axis_index("tp")
    mine = me % SLAB
    z = me // SLAB

    def to_z(step):
        return {"sp": ((z + step + NZ) % NZ) * SLAB + mine}

    def to_slab(step):
        return {"sp": z * SLAB + (mine + step) % SLAB}

    def to_tp(step):
        return {"tp": (tp + step) % TP}

    def remote(src, dst, group, sem, device):
        return pltpu.make_async_remote_copy(
            src_ref=src, dst_ref=dst, send_sem=send_sem.at[group], recv_sem=sem,
            device_id=device, device_id_type=MESH,
        )

    def arrived(ref, sem):
        remote(ref, ref, 0, sem, to_z(1)).wait_recv()

    def left(ref, group):
        remote(ref, ref, group, load_sem.at[0], to_z(1)).wait_send()

    def cols(k):
        return pl.ds(pl.multiple_of(k * W, W), W)

    def rows(first, count):
        return pl.ds(pl.multiple_of(first, 16), count)

    def wo_load(k):
        return pltpu.make_async_copy(w_out_hbm.at[:, cols(k)], wo.at[:, cols(k)], wo_sem.at[k])

    for k in range(NC):
        wo_load(k).start()
    loads = [
        pltpu.make_async_copy(wg_hbm.at[0], wgu.at[:, 0:F], load_sem.at[0]),
        pltpu.make_async_copy(wu_hbm.at[0], wgu.at[:, F : 2 * F], load_sem.at[1]),
        pltpu.make_async_copy(wd_hbm.at[0], wd, load_sem.at[2]),
        pltpu.make_async_copy(sg_hbm, sgu.at[:, 0:F], load_sem.at[3]),
        pltpu.make_async_copy(su_hbm, sgu.at[:, F : 2 * F], load_sem.at[4]),
        pltpu.make_async_copy(sd_hbm, sd, load_sem.at[5]),
    ]
    for load in loads:
        load.start()

    barrier = pltpu.get_barrier_semaphore()
    peers = [to_z(s) for s in range(1, NZ)] + [to_slab(s) for s in range(1, SLAB)]
    peers += [to_tp(s) for s in range(1, TP)]
    for peer in peers:
        pl.semaphore_signal(barrier, inc=1, device_id=peer, device_id_type=MESH)
    cbuf[z] = codes_ref[...]
    pl.semaphore_wait(barrier, len(peers))

    for s in range(1, NZ):
        remote(codes_ref, cbuf.at[z], 0, code_sem, to_z(s)).start()

    def project(k, carry):
        wo_load(k).wait()
        op_all[k] = jnp.dot(
            attn_ref[...], wo[:, cols(k)], preferred_element_type=jnp.float32
        ).astype(jnp.bfloat16)
        for r in range(1, TP):
            src = op_all.at[k, rows(((tp + r) % TP) * ROWS, ROWS), :]
            remote(src, op_in.at[k, (r - 1) * ROWS : r * ROWS, :], 1, op_sem.at[k], to_tp(r)).start()
        return carry

    lax.fori_loop(0, NC, project, 0)

    arrived(cbuf.at[0 : NZ - 1], code_sem)
    slot = lax.broadcasted_iota(jnp.int32, (SLOTS, 128), 0).astype(jnp.float32)
    lane = lax.broadcasted_iota(jnp.int32, (SLOTS, 128), 1).astype(jnp.float32)
    expert = jnp.floor((slot + 0.5) * (1.0 / GROUP))
    inside = slot - expert * GROUP
    source = jnp.floor((inside + 0.5) * (1.0 / CAP))
    want = (z * SLAB * CAP).astype(jnp.float32) + expert * CAP + (inside - source * CAP)
    for q in range(NZ // 2):
        both = cbuf[2 * q] + cbuf[2 * q + 1]
        of_me = source == (2.0 * q + jnp.floor(lane * (1.0 / ROWS)))
        weight = jnp.zeros((SLOTS, 128), jnp.float32)
        hit = jnp.zeros((SLOTS, 128), jnp.float32)
        for j in range(4):
            same = of_me & (both[j : j + 1, :] == want)
            hit = hit + jnp.where(same, 1.0, 0.0)
            weight = weight + jnp.where(same, both[4 + j : 5 + j, :], 0.0)
        place_s[:, q * 128 : (q + 1) * 128] = hit.astype(jnp.bfloat16)
        turned = weight.T
        high = turned.astype(jnp.bfloat16)
        back_hi[q * 128 : (q + 1) * 128, :] = high
        back_lo[q * 128 : (q + 1) * 128, :] = (turned - high.astype(jnp.float32)).astype(jnp.bfloat16)

    def residual(k, square):
        arrived(op_in.at[k], op_sem.at[k])
        total = op_all[k, rows(tp * ROWS, ROWS), :].astype(jnp.float32)
        for r in range(TP - 1):
            total = total + op_in[k, r * ROWS : (r + 1) * ROWS, :].astype(jnp.float32)
        resid = (stream_ref[:, cols(k)].astype(jnp.float32) + total).astype(jnp.bfloat16)
        resid_s[k] = resid
        wide = resid.astype(jnp.float32)
        wide = wide * wide
        for t in range(W // 128):
            square = square + wide[:, t * 128 : (t + 1) * 128]
        return square

    square = lax.fori_loop(0, NC, residual, jnp.zeros((ROWS, 128), jnp.float32))
    inverse = lax.rsqrt(jnp.sum(square, axis=1, keepdims=True) * (1.0 / D) + 1e-06)

    def normalize(k, carry):
        normed = (resid_s[k].astype(jnp.float32) * inverse * gain_ref[:, cols(k)]).astype(jnp.bfloat16)
        zbuf[k, rows(z * ROWS, ROWS), :] = normed
        sh_all[k, 0:ROWS, :] = normed
        return carry

    lax.fori_loop(0, NC, normalize, 0)
    for r in range(1, TP):
        remote(
            sh_all.at[:, 0:ROWS, :], sh_all.at[:, r * ROWS : (r + 1) * ROWS, :], 2, sh_sem, to_tp(r)
        ).start()
    for load in loads:
        load.wait()
    hid_s[...] = jnp.zeros_like(hid_s)

    def pass_rows(k, owner, first, count, way):
        ref = zbuf.at[k, rows(owner * ROWS + first, count), :]
        remote(ref, ref, 3, z_sem.at[k, owner], to_z(way)).start()

    def relay(k, step):
        below, above = (z - step + NZ) % NZ, (z + step) % NZ
        arrived(zbuf.at[k, rows(below * ROWS, ROWS), :], z_sem.at[k, below])
        pass_rows(k, below, 0, ROWS if step < 3 else ROWS // 2, 1)
        arrived(zbuf.at[k, rows(above * ROWS, ROWS), :], z_sem.at[k, above])
        if step < 3:
            pass_rows(k, above, 0, ROWS, -1)
        else:
            pass_rows(k, above, ROWS // 2, ROWS // 2, -1)

    def spread(store, landing, k, sem, group):
        for s in (2, 6, 1, 3, 5, 7, 4):
            src = store.at[k, rows(((mine + s) % SLAB) * GROUP, GROUP), :]
            dst = landing.at[k, rows(mine * GROUP, GROUP), :]
            remote(src, dst, group, sem.at[k], to_slab(s)).start()
        landing[k, rows(mine * GROUP, GROUP), :] = store[k, rows(mine * GROUP, GROUP), :]

    def pack(k):
        far = (z + 4) % NZ
        arrived(zbuf.at[k, rows(far * ROWS, ROWS), :], z_sem.at[k, far])
        ysend[k] = jnp.dot(
            place_s[...], zbuf[k], preferred_element_type=jnp.float32
        ).astype(jnp.bfloat16)
        spread(ysend, xbuf, k, y_sem, 4)

    def enter(k):
        arrived(xbuf.at[k, 0 : SLOTS - GROUP, :], y_sem.at[k])
        hid_s[...] += jnp.dot(xbuf[k], wgu[cols(k), :], preferred_element_type=jnp.float32)

    def shared():
        arrived(sh_all.at[:, ROWS : TP * ROWS, :], sh_sem)

        def gate(k, acc):
            return acc + jnp.dot(sh_all[k], sgu[cols(k), :], preferred_element_type=jnp.float32)

        acc = lax.fori_loop(0, NC, gate, jnp.zeros((TP * ROWS, 2 * F), jnp.float32))
        g = acc[:, 0:F]
        hidden = (g / (1.0 + jnp.exp(-g)) * acc[:, F : 2 * F]).astype(jnp.bfloat16)

        def down(k, carry):
            sh_out[k] = jnp.dot(
                hidden, sd[:, cols(k)], preferred_element_type=jnp.float32
            ).astype(jnp.bfloat16)
            for r in range(1, TP):
                remote(
                    sh_out.at[k, r * ROWS : (r + 1) * ROWS, :],
                    sh_in.at[k, (r - 1) * ROWS : r * ROWS, :],
                    5, shr_sem.at[k], to_tp(TP - r),
                ).start()
            return carry

        lax.fori_loop(0, NC, down, 0)

    def guarded(k, action):
        @pl.when((k >= 0) & (k < NC))
        def _():
            action(k)

    a1, a2, a3, a4, a5 = DISPATCH_LAGS

    def dispatch(t, carry):
        def own(k):
            pass_rows(k, z, 0, ROWS, 1)
            pass_rows(k, z, 0, ROWS, -1)

        guarded(t, own)
        guarded(t - a1, lambda k: relay(k, 1))
        guarded(t - a2, lambda k: relay(k, 2))
        guarded(t - a3, lambda k: relay(k, 3))
        guarded(t - a4, pack)
        guarded(t - a5, enter)

        @pl.when(t == NC)
        def _():
            shared()

        return carry

    lax.fori_loop(0, NC + a5, dispatch, 0)

    g = hid_s[:, 0:F]
    hb_s[...] = (g / (1.0 + jnp.exp(-g)) * hid_s[:, F : 2 * F]).astype(jnp.bfloat16)

    half = ROWS // 2

    def leave(k):
        rsend[k] = jnp.dot(
            hb_s[...], wd[:, cols(k)], preferred_element_type=jnp.float32
        ).astype(jnp.bfloat16)
        spread(rsend, ret, k, r_sem, 6)

    def hand_on(d, k, stage, first, count):
        src = rs_out.at[d, k, stage, first : first + count, :]
        dst = rs_in.at[d, k, stage, first : first + count, :]
        remote(src, dst, 7, rs_sem.at[d, k, stage], to_z(1 - 2 * d)).start()

    def combine(k):
        arrived(ret.at[k, 0 : SLOTS - GROUP, :], r_sem.at[k])
        part_s[k] = jnp.dot(
            back_hi[...], ret[k], preferred_element_type=jnp.float32
        ) + jnp.dot(back_lo[...], ret[k], preferred_element_type=jnp.float32)
        owner = (z + 4) % NZ
        for d in range(2):
            piece = part_s[k, rows(owner * ROWS + d * half, half), :]
            rs_out[d, k, 0, d * half : (d + 1) * half, :] = piece.astype(jnp.bfloat16)
            hand_on(d, k, 0, d * half, half)

    def add_on(k, stage):
        for d in range(2):
            owner = (z + (1 - 2 * d) * (4 - stage) + NZ) % NZ
            first = d * half if stage == 1 else 0
            count = half if stage == 1 else ROWS
            arrived(rs_in.at[d, k, stage - 1, first : first + count, :], rs_sem.at[d, k, stage - 1])
            piece = part_s[k, rows(owner * ROWS + first, count), :]
            piece = piece + rs_in[d, k, stage - 1, first : first + count, :].astype(jnp.float32)
            rs_out[d, k, stage, first : first + count, :] = piece.astype(jnp.bfloat16)
            if stage == 1:
                other = (1 - d) * half
                piece = part_s[k, rows(owner * ROWS + other, half), :]
                rs_out[d, k, stage, other : other + half, :] = piece.astype(jnp.bfloat16)
            hand_on(d, k, stage, 0, ROWS)

    def finish(k):
        total = part_s[k, rows(z * ROWS, ROWS), :]
        for d in range(2):
            arrived(rs_in.at[d, k, 3], rs_sem.at[d, k, 3])
            total = total + rs_in[d, k, 3].astype(jnp.float32)
        arrived(sh_in.at[k], shr_sem.at[k])
        total = total + sh_out[k, 0:ROWS, :].astype(jnp.float32)
        for r in range(TP - 1):
            total = total + sh_in[k, r * ROWS : (r + 1) * ROWS, :].astype(jnp.float32)
        out_ref[:, cols(k)] = (resid_s[k].astype(jnp.float32) + total).astype(jnp.bfloat16)

    b1, b2, b3, b4, b5 = RETURN_LAGS

    def give_back(t, carry):
        guarded(t, leave)
        guarded(t - b4, lambda k: add_on(k, 3))
        guarded(t - b3, lambda k: add_on(k, 2))
        guarded(t - b2, lambda k: add_on(k, 1))
        guarded(t - b1, combine)
        guarded(t - b5, finish)
        return carry

    lax.fori_loop(0, NC + b5, give_back, 0)

    left(cbuf.at[0 : NZ - 1], 0)
    left(op_in, 1)
    left(sh_all.at[:, ROWS : TP * ROWS, :], 2)
    left(zbuf.at[:, 0 : 7 * ROWS, :], 3)
    left(xbuf.at[:, 0 : SLOTS - GROUP, :], 4)
    left(sh_in, 5)
    left(ret.at[:, 0 : SLOTS - GROUP, :], 6)
    left(zbuf.at[:, 0 : 7 * ROWS, :], 7)


def moe(attn_rows, stream_in, norm_gain, codes, w_out, w_gate, w_up, w_down, s_gate, s_up, s_down):
    vmem = pl.BlockSpec(memory_space=pltpu.VMEM)
    hbm = pl.BlockSpec(memory_space=pl.ANY)
    bf, f32 = jnp.bfloat16, jnp.float32
    dma = pltpu.SemaphoreType.DMA
    return pl.pallas_call(
        moe_kernel,
        out_shape=jax.ShapeDtypeStruct((ROWS, D), bf),
        in_specs=[vmem] * 4 + [hbm] * 7,
        out_specs=vmem,
        scratch_shapes=[
            pltpu.VMEM((2 * VD, D), bf),
            pltpu.VMEM((D, 2 * F), bf),
            pltpu.VMEM((F, D), bf),
            pltpu.VMEM((D, 2 * F), bf),
            pltpu.VMEM((F, D), bf),
            pltpu.VMEM((NC, TP * ROWS, W), bf),
            pltpu.VMEM((NC, (TP - 1) * ROWS, W), bf),
            pltpu.VMEM((NC, ROWS, W), bf),
            pltpu.VMEM((NC, NZ * ROWS, W), bf),
            pltpu.VMEM((NZ, 8, 128), f32),
            pltpu.VMEM((SLOTS, NZ * ROWS), bf),
            pltpu.VMEM((NZ * ROWS, SLOTS), bf),
            pltpu.VMEM((NZ * ROWS, SLOTS), bf),
            pltpu.VMEM((NC, SLOTS, W), bf),
            pltpu.VMEM((NC, SLOTS, W), bf),
            pltpu.VMEM((SLOTS, 2 * F), f32),
            pltpu.VMEM((SLOTS, F), bf),
            pltpu.VMEM((NC, SLOTS, W), bf),
            pltpu.VMEM((NC, SLOTS, W), bf),
            pltpu.VMEM((NC, NZ * ROWS, W), f32),
            pltpu.VMEM((2, NC, 4, ROWS, W), bf),
            pltpu.VMEM((2, NC, 4, ROWS, W), bf),
            pltpu.VMEM((NC, TP * ROWS, W), bf),
            pltpu.VMEM((NC, TP * ROWS, W), bf),
            pltpu.VMEM((NC, (TP - 1) * ROWS, W), bf),
            dma((NC,)),
            dma((6,)),
            dma((8,)),
            dma((NC,)),
            dma((NC, NZ)),
            dma,
            dma((NC,)),
            dma((NC,)),
            dma((2, NC, 4)),
            dma,
            dma((NC,)),
        ],
        compiler_params=pltpu.CompilerParams(
            collective_id=1, has_side_effects=True, vmem_limit_bytes=63 * 1024 * 1024
        ),
        name="experts",
    )(attn_rows, stream_in, norm_gain.reshape(1, D), codes, w_out, w_gate, w_up, w_down, s_gate, s_up, s_down)


def slot_codes(routes, route_w):
    flat = routes.reshape(-1)
    count = flat.shape[0]
    hits = (flat[:, None] == jnp.arange(NZ * SLAB, dtype=jnp.int32)[None, :]).astype(jnp.bfloat16)
    at = jnp.arange(count, dtype=jnp.int32)
    earlier = (at[None, :] < at[:, None]).astype(jnp.bfloat16)
    before = jnp.dot(earlier, hits, preferred_element_type=jnp.float32)
    slot = jnp.sum(before * hits.astype(jnp.float32), axis=1)
    codes = flat.astype(jnp.float32) * CAP + slot
    table = jnp.concatenate([codes.reshape(routes.shape).T, route_w.T], axis=0)
    blank = jnp.zeros_like(table)
    odd = (lax.axis_index("sp") // SLAB) % 2 == 1
    return jnp.where(
        odd, jnp.concatenate([blank, table], axis=1), jnp.concatenate([table, blank], axis=1)
    )


def local(
    stream_in,
    q_first,
    q_second,
    k_first,
    k_second,
    values,
    head_lambda,
    w_out,
    norm_gain,
    routes,
    route_w,
    w_gate,
    w_up,
    w_down,
    s_gate,
    s_up,
    s_down,
):
    codes = slot_codes(routes, route_w)
    attn_rows = attention(head_lambda, q_first, q_second, k_first, k_second, values)
    return moe(
        attn_rows, stream_in, norm_gain, codes, w_out, w_gate, w_up, w_down, s_gate, s_up, s_down
    )


def solution(mesh):
    return jax.shard_map(
        local,
        mesh=mesh,
        in_specs=(
            P(("sp", "tp"), None),
            P("sp", "tp"),
            P("sp", "tp"),
            P("sp", "tp"),
            P("sp", "tp"),
            P("sp", "tp"),
            P("tp"),
            P("tp", None),
            P(),
            P(("sp", "tp"), None),
            P(("sp", "tp"), None),
            P("sp", None, None),
            P("sp", None, None),
            P("sp", None, None),
            P(None, "tp"),
            P(None, "tp"),
            P("tp", None),
        ),
        out_specs=P(("sp", "tp"), None),
        check_vma=False,
    )
```

```python
import jax
import jax.numpy as jnp
from jax import lax
from jax.experimental import pallas as pl
from jax.experimental.pallas import tpu as pltpu
from jax.sharding import PartitionSpec as P

HEAD = 128
VD = 256
FLOOR = -1e30
NZ = 8
NY = 4
NCHIP = NZ * NY
BLK = 256
PAIR = 2 * BLK
KVW = 512
LOG2E = 1.4426950408889634

ORDER = sorted(
    [(dz, dy) for dz in (0, 1, -1, 2, -2, 3, -3, 4) for dy in (0, 1, -1, 2)],
    key=lambda a: (abs(a[0]) + abs(a[1]), -abs(a[0]), a),
)
PIECES = ((0, 80, "z", 1), (80, 80, "z", -1), (160, 48, "y", 1), (208, 48, "y", -1))


def step_counts():
    sent = {"z+": 0, "z-": 0, "y+": 0, "y-": 0}
    for dz, dy in ORDER:
        for _, rows, first, way in PIECES:
            for link, go in hops(dz, dy, first, way).items():
                if go:
                    sent[link] += rows
    return sent


def hops(dz, dy, first, way):
    zup = (dz >= 0) & (dz < (4 if way > 0 else 3))
    zdown = (dz <= 0) & (dz > (-3 if way > 0 else -4))
    yup = (dy >= 0) & (dy < (2 if way > 0 else 1))
    ydown = (dy <= 0) & (dy > (-1 if way > 0 else -2))
    if first == "z":
        zup, zdown = zup & (dy == 0), zdown & (dy == 0)
    else:
        yup, ydown = yup & (dz == 0), ydown & (dz == 0)
    return {"z+": zup, "z-": zdown, "y+": yup, "y-": ydown}


def lookup(values, index):
    out = jnp.int32(values[0])
    for k, v in enumerate(values[1:], 1):
        out = jnp.where(index == k, jnp.int32(v), out)
    return out


def attn_kernel(
    lam_ref, q1_hbm, q2_hbm, k1_hbm, k2_hbm, v_hbm, out_ref,
    kv, q_s, m_s, l_s, acc_s, load_sem, send_sem, recv_sem, pair_sem,
):
    me = lax.axis_index("sp")
    c = me % 2
    y = (me // 2) % NY
    z = me // (2 * NY)
    chip = z * NY + y

    def at(zz, yy, cc):
        return {"sp": ((zz + NZ) % NZ) * (2 * NY) + ((yy + NY) % NY) * 2 + cc}

    peers = {
        "z+": at(z + 1, y, c), "z-": at(z - 1, y, c),
        "y+": at(z, y + 1, c), "y-": at(z, y - 1, c),
        "pair": at(z, y, 1 - c),
    }
    links = ("z+", "z-", "y+", "y-", "pair")

    own = pl.multiple_of(chip * PAIR + c * BLK, BLK)
    loads = []
    for k, (src, lo, hi) in enumerate(((k1_hbm, 0, 128), (k2_hbm, 128, 256), (v_hbm, 256, 512))):
        loads.append(pltpu.make_async_copy(src, kv.at[pl.ds(own, BLK), lo:hi], load_sem.at[k]))
        loads[-1].start()

    for k, ref in enumerate((q1_hbm, q2_hbm)):
        for h in range(2):
            loads.append(
                pltpu.make_async_copy(
                    ref.at[:, h * HEAD : (h + 1) * HEAD],
                    q_s.at[k, h * BLK : (h + 1) * BLK, :],
                    load_sem.at[3 + 2 * k + h],
                )
            )
            loads[-1].start()

    barrier = pltpu.get_barrier_semaphore()
    for link in links:
        pl.semaphore_signal(barrier, inc=1, device_id=peers[link], device_id_type=pl.DeviceIdType.MESH)

    scale = HEAD ** (-0.5) * LOG2E
    m_s[...] = jnp.full_like(m_s, FLOOR)
    l_s[...] = jnp.zeros_like(l_s)
    acc_s[...] = jnp.zeros_like(acc_s)

    pl.semaphore_wait(barrier, len(links))
    for copy in loads:
        copy.wait()

    def rows_of(src_chip, core, first, rows):
        return kv.at[pl.ds(pl.multiple_of(src_chip * PAIR + core * BLK + first, 16), rows), :]

    def remote(ref, link, sem):
        return pltpu.make_async_remote_copy(
            src_ref=ref, dst_ref=ref, send_sem=send_sem.at[links.index(link)], recv_sem=sem,
            device_id=peers[link], device_id_type=pl.DeviceIdType.MESH,
        )

    def forward(dz, dy, src_chip):
        for first_row, rows, first, way in PIECES:
            for link, go in hops(dz, dy, first, way).items():

                @pl.when(go)
                def _():
                    remote(rows_of(src_chip, c, first_row, rows), link, recv_sem.at[src_chip]).start()

        remote(rows_of(src_chip, c, 0, BLK), "pair", pair_sem.at[src_chip]).start()

    def attend(src_chip, masked):
        base = pl.multiple_of(src_chip * PAIR, PAIR)
        value = kv[pl.ds(base, PAIR), 256:512]
        for k in range(2):
            key = kv[pl.ds(base, PAIR), k * HEAD : (k + 1) * HEAD]
            scores = lax.dot_general(
                q_s[k], key, (((1,), (1,)), ((), ())), preferred_element_type=jnp.float32
            ) * scale
            if masked:
                q_pos = lax.broadcasted_iota(jnp.int32, scores.shape, 0) % BLK + c * BLK
                k_pos = lax.broadcasted_iota(jnp.int32, scores.shape, 1)
                scores = jnp.where(k_pos <= q_pos, scores, FLOOR)
            old = m_s[k]
            new = jnp.maximum(old, jnp.max(scores, axis=1, keepdims=True))
            fade = jnp.exp2(old - new)
            weights = jnp.exp2(scores - jnp.tile(new, (1, PAIR // 128)))
            if masked:
                weights = jnp.where(k_pos <= q_pos, weights, 0.0)
            part = weights[:, 0:128]
            for t in range(1, PAIR // 128):
                part = part + weights[:, t * 128 : (t + 1) * 128]
            m_s[k] = new
            l_s[k] = l_s[k] * fade + part
            acc_s[k] = acc_s[k] * jnp.tile(fade, (1, VD // 128)) + jnp.dot(
                weights.astype(jnp.bfloat16), value, preferred_element_type=jnp.float32
            )

    forward(jnp.int32(0), jnp.int32(0), chip)

    dz_table = [o[0] for o in ORDER]
    dy_table = [o[1] for o in ORDER]

    def place(e):
        dz, dy = lookup(dz_table, e), lookup(dy_table, e)
        return dz, dy, ((z - dz + NZ) % NZ) * NY + (y - dy + NY) % NY

    def step(e, carry):
        @pl.when(e < NCHIP)
        def _():
            dz, dy, src = place(e)
            remote(rows_of(src, c, 0, BLK), "z+", recv_sem.at[src]).wait_recv()
            forward(dz, dy, src)

        _, _, last = place(e - 1)
        remote(rows_of(last, 1 - c, 0, BLK), "pair", pair_sem.at[last]).wait_recv()

        @pl.when(e == 1)
        def _():
            attend(chip, True)

        @pl.when((e > 1) & (last < chip))
        def _():
            attend(last, False)

        return carry

    lax.fori_loop(1, NCHIP + 1, step, 0)

    head_rows = []
    for k in range(2):
        total = jnp.sum(l_s[k], axis=1, keepdims=True)
        head_rows.append(acc_s[k] / total)
    for h in range(2):
        span = slice(h * BLK, (h + 1) * BLK)
        head = head_rows[0][span] - lam_ref[h] * head_rows[1][span]
        head = head * lax.rsqrt(jnp.mean(head * head, axis=1, keepdims=True) + 1e-05)
        out_ref[:, h * VD : (h + 1) * VD] = head.astype(jnp.bfloat16)

    for link, rows in step_counts().items():
        remote(kv.at[pl.ds(0, rows), :], link, recv_sem.at[0]).wait_send()
    remote(kv.at[pl.ds(0, NCHIP * BLK), :], "pair", recv_sem.at[0]).wait_send()


def attention(head_lambda, q_first, q_second, k_first, k_second, values):
    vmem = pl.BlockSpec(memory_space=pltpu.VMEM)
    hbm = pl.BlockSpec(memory_space=pl.ANY)
    return pl.pallas_call(
        attn_kernel,
        out_shape=jax.ShapeDtypeStruct((BLK, 2 * VD), jnp.bfloat16),
        in_specs=[pl.BlockSpec(memory_space=pltpu.SMEM)] + [hbm] * 5,
        out_specs=vmem,
        scratch_shapes=[
            pltpu.VMEM((NCHIP * PAIR, KVW), jnp.bfloat16),
            pltpu.VMEM((2, 2 * BLK, HEAD), jnp.bfloat16),
            pltpu.VMEM((2, 2 * BLK, 128), jnp.float32),
            pltpu.VMEM((2, 2 * BLK, 128), jnp.float32),
            pltpu.VMEM((2, 2 * BLK, VD), jnp.float32),
            pltpu.SemaphoreType.DMA((7,)),
            pltpu.SemaphoreType.DMA((5,)),
            pltpu.SemaphoreType.DMA((NCHIP,)),
            pltpu.SemaphoreType.DMA((NCHIP,)),
        ],
        compiler_params=pltpu.CompilerParams(
            collective_id=0, has_side_effects=True, vmem_limit_bytes=63 * 1024 * 1024
        ),
        name="attend",
    )(head_lambda, q_first, q_second, k_first, k_second, values)


D = 4096
ROWS = 64
TP = 4
TOPK = 4
SLAB = 2 * NY
CAP = 6
GROUP = NZ * CAP
SLOTS = SLAB * GROUP
NC = 16
W = D // NC
F = 128
MESH = pl.DeviceIdType.MESH
SUM_LAG, RESID_LAG = 3, 5
HOP_LAGS = tuple(RESID_LAG + n for n in (3, 4, 5))
PACK_LAG, ENTER_LAG = RESID_LAG + 6, RESID_LAG + 9
SHARE_LAG = RESID_LAG + 4
RETURN_LAGS = (2, 4, 6, 9, 11)


def moe_kernel(
    attn_hbm, stream_hbm, gain_hbm, routes_ref, route_w_ref,
    w_out_hbm, wg_hbm, wu_hbm, wd_hbm, sg_hbm, su_hbm, sd_hbm,
    out_ref,
    attn_s, stream_s, gain_s, wo, wgu, wd, sgu, sd,
    op_all, op_out, op_in, resid_s, square_s, zbuf, cbuf, place_s, back_hi, back_lo,
    turn_s, inv_own, inv_z, inv_send, inv_slot, inv_sh,
    ysend, xbuf, hid_s, hb_s, rsend, ret, part_s, rs_out, rs_in,
    sh_all, sh_out, sh_pass, sh_in,
    wo_sem, load_sem, send_sem, op_sem, z_sem, code_sem, y_sem, r_sem, rs_sem,
    sh_sem, shr_sem, inv_z_sem, inv_slot_sem, inv_sh_sem,
):
    me = lax.axis_index("sp")
    tp = lax.axis_index("tp")
    mine = me % SLAB
    z = me // SLAB
    half = ROWS // 2

    def to_z(step):
        return {"sp": ((z + step + NZ) % NZ) * SLAB + mine}

    def to_slab(step):
        return {"sp": z * SLAB + (mine + step) % SLAB}

    def to_tp(step):
        return {"tp": (tp + step + TP) % TP}

    def remote(src, dst, group, sem, device):
        return pltpu.make_async_remote_copy(
            src_ref=src, dst_ref=dst, send_sem=send_sem.at[group], recv_sem=sem,
            device_id=device, device_id_type=MESH,
        )

    def arrived(ref, sem):
        remote(ref, ref, 0, sem, to_z(1)).wait_recv()

    def left(ref, group):
        remote(ref, ref, group, load_sem.at[0], to_z(1)).wait_send()

    def cols(k):
        return pl.ds(pl.multiple_of(k * W, W), W)

    def rows(first, count):
        return pl.ds(pl.multiple_of(first, 16), count)

    def wo_load(k):
        return pltpu.make_async_copy(w_out_hbm.at[:, cols(k)], wo.at[:, cols(k)], wo_sem.at[k])

    early = [
        pltpu.make_async_copy(attn_hbm, attn_s, load_sem.at[6]),
        pltpu.make_async_copy(stream_hbm, stream_s, load_sem.at[7]),
        pltpu.make_async_copy(gain_hbm, gain_s, load_sem.at[8]),
    ]
    for load in early:
        load.start()
    for k in range(NC):
        wo_load(k).start()
    loads = [
        pltpu.make_async_copy(wg_hbm.at[0], wgu.at[:, 0:F], load_sem.at[0]),
        pltpu.make_async_copy(wu_hbm.at[0], wgu.at[:, F : 2 * F], load_sem.at[1]),
        pltpu.make_async_copy(wd_hbm.at[0], wd, load_sem.at[2]),
        pltpu.make_async_copy(sg_hbm, sgu.at[:, 0:F], load_sem.at[3]),
        pltpu.make_async_copy(su_hbm, sgu.at[:, F : 2 * F], load_sem.at[4]),
        pltpu.make_async_copy(sd_hbm, sd, load_sem.at[5]),
    ]
    for load in loads:
        load.start()

    barrier = pltpu.get_barrier_semaphore()
    peers = [to_z(s) for s in range(1, NZ)] + [to_slab(s) for s in range(1, SLAB)]
    peers += [to_tp(s) for s in range(1, TP)]
    for peer in peers:
        pl.semaphore_signal(barrier, inc=1, device_id=peer, device_id_type=MESH)

    names = lax.broadcasted_iota(jnp.int32, (NZ * SLAB, ROWS), 0)
    hits = jnp.zeros((NZ * SLAB, ROWS), jnp.float32)
    for j in range(TOPK):
        hits = hits + jnp.where(routes_ref[j : j + 1, :] == names, 1.0, 0.0)
    upper = (
        lax.broadcasted_iota(jnp.int32, (ROWS, ROWS), 0)
        < lax.broadcasted_iota(jnp.int32, (ROWS, ROWS), 1)
    )
    before = jnp.dot(
        hits.astype(jnp.bfloat16),
        jnp.where(upper, 1.0, 0.0).astype(jnp.bfloat16),
        preferred_element_type=jnp.float32,
    )
    table = []
    for j in range(TOPK):
        chosen = routes_ref[j : j + 1, :]
        taken = jnp.sum(jnp.where(chosen == names, before, 0.0), axis=0, keepdims=True)
        table.append(chosen.astype(jnp.float32) * CAP + taken)
    for j in range(TOPK):
        table.append(route_w_ref[j : j + 1, :])
    table = jnp.concatenate(table, axis=0)
    odd = (z % 2).astype(jnp.float32)
    cbuf[z] = jnp.concatenate([table * (1.0 - odd), table * odd], axis=1)
    turn_s[...] = jnp.zeros_like(turn_s)
    square_s[...] = jnp.zeros_like(square_s)
    hid_s[...] = jnp.zeros_like(hid_s)

    pl.semaphore_wait(barrier, len(peers))
    for s in range(1, NZ):
        remote(cbuf.at[z], cbuf.at[z], 0, code_sem, to_z(s)).start()
    for load in early:
        load.wait()

    def ring_out(d, stage, first, count, k, src, group, landing, sem):
        dst = landing.at[d, k, stage, first : first + count, :]
        remote(src, dst, group, sem.at[d, k, stage], to_tp(1 - 2 * d)).start()

    def ring_first(k, table_ref, landing, group, sem):
        for d in range(2):
            src = table_ref.at[k, rows(((tp + 2) % TP) * ROWS + d * half, half), :]
            ring_out(d, 0, d * half, half, k, src, group, landing, sem)

    def ring_second(k, table_ref, passing, landing, group, sem):
        for d in range(2):
            first, other = d * half, (1 - d) * half
            owner = (tp + 1 - 2 * d + TP) % TP
            arrived(landing.at[d, k, 0, first : first + half, :], sem.at[d, k, 0])
            piece = table_ref[k, rows(owner * ROWS + first, half), :].astype(jnp.float32)
            piece = piece + landing[d, k, 0, first : first + half, :].astype(jnp.float32)
            passing[d, k, first : first + half, :] = piece.astype(jnp.bfloat16)
            passing[d, k, other : other + half, :] = table_ref[k, rows(owner * ROWS + other, half), :]
            ring_out(d, 1, 0, ROWS, k, passing.at[d, k], group, landing, sem)

    def ring_total(k, table_ref, landing, sem):
        total = table_ref[k, rows(tp * ROWS, ROWS), :].astype(jnp.float32)
        for d in range(2):
            arrived(landing.at[d, k, 1], sem.at[d, k, 1])
            total = total + landing[d, k, 1].astype(jnp.float32)
        return total

    def project(k):
        wo_load(k).wait()
        op_all[k] = jnp.dot(
            attn_s[...], wo[:, cols(k)], preferred_element_type=jnp.float32
        ).astype(jnp.bfloat16)
        ring_first(k, op_all, op_in, 1, op_sem)

    def pass_rows(k, owner, first, count, way):
        ref = zbuf.at[k, rows(owner * ROWS + first, count), :]
        remote(ref, ref, 3, z_sem.at[k, owner], to_z(way)).start()

    def share_rows(k, owner, first, count, way):
        ref = sh_all.at[k, rows(owner * ROWS + first, count), :]
        remote(ref, ref, 2, sh_sem.at[k, owner], to_tp(way)).start()

    def residual(k):
        total = ring_total(k, op_all, op_in, op_sem)
        resid = (stream_s[:, cols(k)].astype(jnp.float32) + total).astype(jnp.bfloat16)
        resid_s[k] = resid
        wide = resid.astype(jnp.float32)
        gain = jnp.concatenate(
            [gain_s[pl.ds(k * (W // 128) + t, 1), :] for t in range(W // 128)], axis=1
        )
        scaled = (wide * gain).astype(jnp.bfloat16)
        zbuf[k, rows(z * ROWS, ROWS), :] = scaled
        sh_all[k, rows(tp * ROWS, ROWS), :] = scaled
        for way in (1, -1):
            pass_rows(k, z, 0, ROWS, way)
            share_rows(k, tp, 0, ROWS, way)
        wide = wide * wide
        square = square_s[...]
        for t in range(W // 128):
            square = square + wide[:, t * 128 : (t + 1) * 128]
        square_s[...] = square

    def send_inverse():
        mean = jnp.sum(square_s[...], axis=1, keepdims=True) * (1.0 / D)
        inverse = jnp.broadcast_to(lax.rsqrt(mean + 1e-06), (ROWS, 128))
        inv_sh[rows(tp * ROWS, ROWS), :] = inverse
        turn_s[rows((z % 2) * ROWS, ROWS), :] = inverse
        inv_own[...] = turn_s[...].T[0:8, :]
        inv_z[z] = inv_own[...]
        for s in range(1, NZ):
            remote(inv_own, inv_z.at[z], 8, inv_z_sem, to_z(s)).start()
        own = inv_sh.at[rows(tp * ROWS, ROWS), :]
        for r in range(1, TP):
            remote(own, own, 9, inv_sh_sem, to_tp(r)).start()

    def spread_inverse():
        arrived(inv_z.at[0 : NZ - 1], inv_z_sem)
        total = jnp.zeros((SLOTS, 128), jnp.float32)
        for q in range(NZ // 2):
            both = inv_z[2 * q] + inv_z[2 * q + 1]
            total = total + place_s[:, q * 128 : (q + 1) * 128].astype(jnp.float32) * both[0:1, :]
        inv_send[...] = jnp.broadcast_to(jnp.sum(total, axis=1, keepdims=True), (SLOTS, 128))
        land = inv_slot.at[rows(mine * GROUP, GROUP), :]
        for s in range(1, SLAB):
            src = inv_send.at[rows(((mine + s) % SLAB) * GROUP, GROUP), :]
            remote(src, land, 10, inv_slot_sem, to_slab(s)).start()
        inv_slot[rows(mine * GROUP, GROUP), :] = inv_send[rows(mine * GROUP, GROUP), :]

    def places():
        arrived(cbuf.at[0 : NZ - 1], code_sem)
        slot = lax.broadcasted_iota(jnp.int32, (SLOTS, 128), 0).astype(jnp.float32)
        lane = lax.broadcasted_iota(jnp.int32, (SLOTS, 128), 1).astype(jnp.float32)
        expert = jnp.floor((slot + 0.5) * (1.0 / GROUP))
        inside = slot - expert * GROUP
        source = jnp.floor((inside + 0.5) * (1.0 / CAP))
        want = (z * SLAB * CAP).astype(jnp.float32) + expert * CAP + (inside - source * CAP)
        for q in range(NZ // 2):
            both = cbuf[2 * q] + cbuf[2 * q + 1]
            of_me = source == (2.0 * q + jnp.floor(lane * (1.0 / ROWS)))
            weight = jnp.zeros((SLOTS, 128), jnp.float32)
            hit = jnp.zeros((SLOTS, 128), jnp.float32)
            for j in range(TOPK):
                same = of_me & (both[j : j + 1, :] == want)
                hit = hit + jnp.where(same, 1.0, 0.0)
                weight = weight + jnp.where(same, both[TOPK + j : TOPK + j + 1, :], 0.0)
            place_s[:, q * 128 : (q + 1) * 128] = hit.astype(jnp.bfloat16)
            turned = weight.T
            high = turned.astype(jnp.bfloat16)
            back_hi[q * 128 : (q + 1) * 128, :] = high
            back_lo[q * 128 : (q + 1) * 128, :] = (turned - high.astype(jnp.float32)).astype(
                jnp.bfloat16
            )

    def relay(k, step):
        below, above = (z - step + NZ) % NZ, (z + step) % NZ
        arrived(zbuf.at[k, rows(below * ROWS, ROWS), :], z_sem.at[k, below])
        pass_rows(k, below, 0, ROWS if step < 3 else half, 1)
        arrived(zbuf.at[k, rows(above * ROWS, ROWS), :], z_sem.at[k, above])
        if step < 3:
            pass_rows(k, above, 0, ROWS, -1)
        else:
            pass_rows(k, above, half, half, -1)

    def share(k):
        below, above = (tp + TP - 1) % TP, (tp + 1) % TP
        arrived(sh_all.at[k, rows(below * ROWS, ROWS), :], sh_sem.at[k, below])
        share_rows(k, below, 0, half, 1)
        arrived(sh_all.at[k, rows(above * ROWS, ROWS), :], sh_sem.at[k, above])
        share_rows(k, above, half, half, -1)

    def spread(store, landing, k, sem, group):
        for s in (2, 6, 1, 3, 5, 7, 4):
            src = store.at[k, rows(((mine + s) % SLAB) * GROUP, GROUP), :]
            dst = landing.at[k, rows(mine * GROUP, GROUP), :]
            remote(src, dst, group, sem.at[k], to_slab(s)).start()
        landing[k, rows(mine * GROUP, GROUP), :] = store[k, rows(mine * GROUP, GROUP), :]

    def pack(k):
        far = (z + 4) % NZ
        arrived(zbuf.at[k, rows(far * ROWS, ROWS), :], z_sem.at[k, far])
        ysend[k] = jnp.dot(
            place_s[...], zbuf[k], preferred_element_type=jnp.float32
        ).astype(jnp.bfloat16)
        spread(ysend, xbuf, k, y_sem, 4)

    def enter(k):
        arrived(xbuf.at[k, 0 : SLOTS - GROUP, :], y_sem.at[k])
        hid_s[...] += jnp.dot(xbuf[k], wgu[cols(k), :], preferred_element_type=jnp.float32)

    def gated(sums, inverse):
        g = sums[:, 0:F] * inverse
        return (g / (1.0 + jnp.exp(-g)) * (sums[:, F : 2 * F] * inverse)).astype(jnp.bfloat16)

    def shared():
        def gate(k, acc):
            far = (tp + 2) % TP
            arrived(sh_all.at[k, rows(far * ROWS, ROWS), :], sh_sem.at[k, far])
            return acc + jnp.dot(sh_all[k], sgu[cols(k), :], preferred_element_type=jnp.float32)

        acc = lax.fori_loop(0, NC, gate, jnp.zeros((TP * ROWS, 2 * F), jnp.float32))
        arrived(inv_sh.at[0 : (TP - 1) * ROWS, :], inv_sh_sem)
        hidden = gated(acc, inv_sh[...])

        def down(k, carry):
            sh_out[k] = jnp.dot(
                hidden, sd[:, cols(k)], preferred_element_type=jnp.float32
            ).astype(jnp.bfloat16)
            ring_first(k, sh_out, sh_in, 5, shr_sem)
            return carry

        lax.fori_loop(0, NC, down, 0)

    def guarded(k, action):
        @pl.when((k >= 0) & (k < NC))
        def _():
            action(k)

    def way_out(t, carry):
        guarded(t, project)

        @pl.when(t == 1)
        def _():
            places()
            for load in loads:
                load.wait()

        guarded(t - SUM_LAG, lambda k: ring_second(k, op_all, op_out, op_in, 1, op_sem))
        for step in (1, 2, 3):
            guarded(t - HOP_LAGS[step - 1], lambda k, step=step: relay(k, step))
        guarded(t - RESID_LAG, residual)

        @pl.when(t == NC - 1 + RESID_LAG)
        def _():
            send_inverse()

        guarded(t - SHARE_LAG, share)
        guarded(t - PACK_LAG, pack)
        guarded(t - ENTER_LAG, enter)

        @pl.when(t == NC + 1 + RESID_LAG)
        def _():
            spread_inverse()

        @pl.when(t == NC + 2 + SHARE_LAG)
        def _():
            shared()

        return carry

    lax.fori_loop(0, NC + ENTER_LAG, way_out, 0)

    arrived(inv_slot.at[0 : SLOTS - GROUP, :], inv_slot_sem)
    hb_s[...] = gated(hid_s[...], inv_slot[...])

    def leave(k):
        rsend[k] = jnp.dot(
            hb_s[...], wd[:, cols(k)], preferred_element_type=jnp.float32
        ).astype(jnp.bfloat16)
        spread(rsend, ret, k, r_sem, 6)

    def hand_on(d, k, stage, first, count):
        src = rs_out.at[d, k, stage, first : first + count, :]
        dst = rs_in.at[d, k, stage, first : first + count, :]
        remote(src, dst, 7, rs_sem.at[d, k, stage], to_z(1 - 2 * d)).start()

    def combine(k):
        arrived(ret.at[k, 0 : SLOTS - GROUP, :], r_sem.at[k])
        part_s[k] = jnp.dot(
            back_hi[...], ret[k], preferred_element_type=jnp.float32
        ) + jnp.dot(back_lo[...], ret[k], preferred_element_type=jnp.float32)
        owner = (z + 4) % NZ
        for d in range(2):
            piece = part_s[k, rows(owner * ROWS + d * half, half), :]
            rs_out[d, k, 0, d * half : (d + 1) * half, :] = piece.astype(jnp.bfloat16)
            hand_on(d, k, 0, d * half, half)

    def add_on(k, stage):
        for d in range(2):
            owner = (z + (1 - 2 * d) * (4 - stage) + NZ) % NZ
            first = d * half if stage == 1 else 0
            count = half if stage == 1 else ROWS
            arrived(rs_in.at[d, k, stage - 1, first : first + count, :], rs_sem.at[d, k, stage - 1])
            piece = part_s[k, rows(owner * ROWS + first, count), :]
            piece = piece + rs_in[d, k, stage - 1, first : first + count, :].astype(jnp.float32)
            rs_out[d, k, stage, first : first + count, :] = piece.astype(jnp.bfloat16)
            if stage == 1:
                other = (1 - d) * half
                piece = part_s[k, rows(owner * ROWS + other, half), :]
                rs_out[d, k, stage, other : other + half, :] = piece.astype(jnp.bfloat16)
            hand_on(d, k, stage, 0, ROWS)

    def finish(k):
        total = part_s[k, rows(z * ROWS, ROWS), :]
        for d in range(2):
            arrived(rs_in.at[d, k, 3], rs_sem.at[d, k, 3])
            total = total + rs_in[d, k, 3].astype(jnp.float32)
        total = total + ring_total(k, sh_out, sh_in, shr_sem)
        out_ref[:, cols(k)] = (resid_s[k].astype(jnp.float32) + total).astype(jnp.bfloat16)

    b1, b2, b3, b4, b5 = RETURN_LAGS

    def give_back(t, carry):
        guarded(t, leave)
        guarded(t - b4, lambda k: add_on(k, 3))
        guarded(t - b3, lambda k: add_on(k, 2))
        guarded(t - b2, lambda k: add_on(k, 1))
        guarded(t - b1, combine)
        guarded(t - b1, lambda k: ring_second(k, sh_out, sh_pass, sh_in, 5, shr_sem))
        guarded(t - b5, finish)
        return carry

    lax.fori_loop(0, NC + b5, give_back, 0)

    left(cbuf.at[0 : NZ - 1], 0)
    left(sh_all.at[:, 0 : 3 * ROWS, :], 1)
    left(sh_all.at[:, 0 : 3 * ROWS, :], 2)
    left(zbuf.at[:, 0 : 7 * ROWS, :], 3)
    left(xbuf.at[:, 0 : SLOTS - GROUP, :], 4)
    left(sh_all.at[:, 0 : 3 * ROWS, :], 5)
    left(ret.at[:, 0 : SLOTS - GROUP, :], 6)
    left(zbuf.at[:, 0 : 7 * ROWS, :], 7)
    left(inv_z.at[0 : NZ - 1], 8)
    left(inv_sh.at[0 : (TP - 1) * ROWS, :], 9)
    left(inv_slot.at[0 : SLOTS - GROUP, :], 10)


def moe(
    attn_rows, stream_in, norm_gain, routes, route_w, w_out, w_gate, w_up, w_down, s_gate, s_up, s_down
):
    vmem = pl.BlockSpec(memory_space=pltpu.VMEM)
    hbm = pl.BlockSpec(memory_space=pl.ANY)
    bf, f32 = jnp.bfloat16, jnp.float32
    dma = pltpu.SemaphoreType.DMA
    return pl.pallas_call(
        moe_kernel,
        out_shape=jax.ShapeDtypeStruct((ROWS, D), bf),
        in_specs=[hbm] * 3 + [vmem] * 2 + [hbm] * 7,
        out_specs=vmem,
        scratch_shapes=[
            pltpu.VMEM((TP * ROWS, 2 * VD), bf),
            pltpu.VMEM((ROWS, D), bf),
            pltpu.VMEM((D // 128, 128), f32),
            pltpu.VMEM((2 * VD, D), bf),
            pltpu.VMEM((D, 2 * F), bf),
            pltpu.VMEM((F, D), bf),
            pltpu.VMEM((D, 2 * F), bf),
            pltpu.VMEM((F, D), bf),
            pltpu.VMEM((NC, TP * ROWS, W), bf),
            pltpu.VMEM((2, NC, ROWS, W), bf),
            pltpu.VMEM((2, NC, 2, ROWS, W), bf),
            pltpu.VMEM((NC, ROWS, W), bf),
            pltpu.VMEM((ROWS, 128), f32),
            pltpu.VMEM((NC, NZ * ROWS, W), bf),
            pltpu.VMEM((NZ, 8, 128), f32),
            pltpu.VMEM((SLOTS, NZ * ROWS), bf),
            pltpu.VMEM((NZ * ROWS, SLOTS), bf),
            pltpu.VMEM((NZ * ROWS, SLOTS), bf),
            pltpu.VMEM((2 * ROWS, 128), f32),
            pltpu.VMEM((8, 128), f32),
            pltpu.VMEM((NZ, 8, 128), f32),
            pltpu.VMEM((SLOTS, 128), f32),
            pltpu.VMEM((SLOTS, 128), f32),
            pltpu.VMEM((TP * ROWS, 128), f32),
            pltpu.VMEM((NC, SLOTS, W), bf),
            pltpu.VMEM((NC, SLOTS, W), bf),
            pltpu.VMEM((SLOTS, 2 * F), f32),
            pltpu.VMEM((SLOTS, F), bf),
            pltpu.VMEM((NC, SLOTS, W), bf),
            pltpu.VMEM((NC, SLOTS, W), bf),
            pltpu.VMEM((NC, NZ * ROWS, W), f32),
            pltpu.VMEM((2, NC, 4, ROWS, W), bf),
            pltpu.VMEM((2, NC, 4, ROWS, W), bf),
            pltpu.VMEM((NC, TP * ROWS, W), bf),
            pltpu.VMEM((NC, TP * ROWS, W), bf),
            pltpu.VMEM((2, NC, ROWS, W), bf),
            pltpu.VMEM((2, NC, 2, ROWS, W), bf),
            dma((NC,)),
            dma((9,)),
            dma((11,)),
            dma((2, NC, 2)),
            dma((NC, NZ)),
            dma,
            dma((NC,)),
            dma((NC,)),
            dma((2, NC, 4)),
            dma((NC, TP)),
            dma((2, NC, 2)),
            dma,
            dma,
            dma,
        ],
        compiler_params=pltpu.CompilerParams(
            collective_id=1, has_side_effects=True, vmem_limit_bytes=67043328
        ),
        name="experts",
    )(
        attn_rows, stream_in, norm_gain.reshape(D // 128, 128), routes.T, route_w.T,
        w_out, w_gate, w_up, w_down, s_gate, s_up, s_down,
    )


def local(
    stream_in,
    q_first,
    q_second,
    k_first,
    k_second,
    values,
    head_lambda,
    w_out,
    norm_gain,
    routes,
    route_w,
    w_gate,
    w_up,
    w_down,
    s_gate,
    s_up,
    s_down,
):
    attn_rows = attention(head_lambda, q_first, q_second, k_first, k_second, values)
    return moe(
        attn_rows, stream_in, norm_gain, routes, route_w, w_out, w_gate, w_up, w_down, s_gate, s_up, s_down
    )


def solution(mesh):
    return jax.shard_map(
        local,
        mesh=mesh,
        in_specs=(
            P(("sp", "tp"), None),
            P("sp", "tp"),
            P("sp", "tp"),
            P("sp", "tp"),
            P("sp", "tp"),
            P("sp", "tp"),
            P("tp"),
            P("tp", None),
            P(),
            P(("sp", "tp"), None),
            P(("sp", "tp"), None),
            P("sp", None, None),
            P("sp", None, None),
            P("sp", None, None),
            P(None, "tp"),
            P(None, "tp"),
            P("tp", None),
        ),
        out_specs=P(("sp", "tp"), None),
        check_vma=False,
    )
```

```python
import jax
import jax.numpy as jnp
from jax import lax
from jax.experimental import pallas as pl
from jax.experimental.pallas import tpu as pltpu
from jax.sharding import PartitionSpec as P

HEAD = 128
VD = 256
FLOOR = -1e30
NZ = 8
NY = 4
NCHIP = NZ * NY
BLK = 256
PAIR = 2 * BLK
KVW = 512
LOG2E = 1.4426950408889634

ORDER = sorted(
    [(dz, dy) for dz in (0, 1, -1, 2, -2, 3, -3, 4) for dy in (0, 1, -1, 2)],
    key=lambda a: (abs(a[0]) + abs(a[1]), -abs(a[0]), a),
)
PIECES = ((0, 80, "z", 1), (80, 80, "z", -1), (160, 48, "y", 1), (208, 48, "y", -1))


def step_counts():
    sent = {"z+": 0, "z-": 0, "y+": 0, "y-": 0}
    for dz, dy in ORDER:
        for _, rows, first, way in PIECES:
            for link, go in hops(dz, dy, first, way).items():
                if go:
                    sent[link] += rows
    return sent


def hops(dz, dy, first, way):
    zup = (dz >= 0) & (dz < (4 if way > 0 else 3))
    zdown = (dz <= 0) & (dz > (-3 if way > 0 else -4))
    yup = (dy >= 0) & (dy < (2 if way > 0 else 1))
    ydown = (dy <= 0) & (dy > (-1 if way > 0 else -2))
    if first == "z":
        zup, zdown = zup & (dy == 0), zdown & (dy == 0)
    else:
        yup, ydown = yup & (dz == 0), ydown & (dz == 0)
    return {"z+": zup, "z-": zdown, "y+": yup, "y-": ydown}


def lookup(values, index):
    out = jnp.int32(values[0])
    for k, v in enumerate(values[1:], 1):
        out = jnp.where(index == k, jnp.int32(v), out)
    return out


def attn_kernel(
    lam_ref, q1_hbm, q2_hbm, k1_hbm, k2_hbm, v_hbm, routes_ref, route_w_ref,
    out_ref, place_ref, high_ref, low_ref,
    kv, q_s, m_s, l_s, acc_s, load_sem, send_sem, recv_sem, pair_sem, cbuf, code_sem,
):
    me = lax.axis_index("sp")
    c = me % 2
    y = (me // 2) % NY
    z = me // (2 * NY)
    chip = z * NY + y

    def at(zz, yy, cc):
        return {"sp": ((zz + NZ) % NZ) * (2 * NY) + ((yy + NY) % NY) * 2 + cc}

    peers = {
        "z+": at(z + 1, y, c), "z-": at(z - 1, y, c),
        "y+": at(z, y + 1, c), "y-": at(z, y - 1, c),
        "pair": at(z, y, 1 - c),
    }
    links = ("z+", "z-", "y+", "y-", "pair")
    far = [at(z + step, y, c) for step in range(2, NZ - 1)]

    own = pl.multiple_of(chip * PAIR + c * BLK, BLK)
    loads = []
    for k, (src, lo, hi) in enumerate(((k1_hbm, 0, 128), (k2_hbm, 128, 256), (v_hbm, 256, 512))):
        loads.append(pltpu.make_async_copy(src, kv.at[pl.ds(own, BLK), lo:hi], load_sem.at[k]))
        loads[-1].start()

    for k, ref in enumerate((q1_hbm, q2_hbm)):
        for h in range(2):
            loads.append(
                pltpu.make_async_copy(
                    ref.at[:, h * HEAD : (h + 1) * HEAD],
                    q_s.at[k, h * BLK : (h + 1) * BLK, :],
                    load_sem.at[3 + 2 * k + h],
                )
            )
            loads[-1].start()

    barrier = pltpu.get_barrier_semaphore()
    for link in links:
        pl.semaphore_signal(barrier, inc=1, device_id=peers[link], device_id_type=pl.DeviceIdType.MESH)
    for peer in far:
        pl.semaphore_signal(barrier, inc=1, device_id=peer, device_id_type=pl.DeviceIdType.MESH)

    scale = HEAD ** (-0.5) * LOG2E
    m_s[...] = jnp.full_like(m_s, FLOOR)
    l_s[...] = jnp.zeros_like(l_s)
    acc_s[...] = jnp.zeros_like(acc_s)

    names = lax.broadcasted_iota(jnp.int32, (NZ * SLAB, ROWS), 0)
    hits = jnp.zeros((NZ * SLAB, ROWS), jnp.float32)
    for j in range(TOPK):
        hits = hits + jnp.where(routes_ref[j : j + 1, :] == names, 1.0, 0.0)
    upper = (
        lax.broadcasted_iota(jnp.int32, (ROWS, ROWS), 0)
        < lax.broadcasted_iota(jnp.int32, (ROWS, ROWS), 1)
    )
    before = jnp.dot(
        hits.astype(jnp.bfloat16),
        jnp.where(upper, 1.0, 0.0).astype(jnp.bfloat16),
        preferred_element_type=jnp.float32,
    )
    table = []
    for j in range(TOPK):
        chosen = routes_ref[j : j + 1, :]
        taken = jnp.sum(jnp.where(chosen == names, before, 0.0), axis=0, keepdims=True)
        table.append(chosen.astype(jnp.float32) * CAP + taken)
    for j in range(TOPK):
        table.append(route_w_ref[j : j + 1, :])
    table = jnp.concatenate(table, axis=0)
    odd = (z % 2).astype(jnp.float32)
    cbuf[z] = jnp.concatenate([table * (1.0 - odd), table * odd], axis=1)

    pl.semaphore_wait(barrier, len(links) + len(far))
    for copy in loads:
        copy.wait()

    def rows_of(src_chip, core, first, rows):
        return kv.at[pl.ds(pl.multiple_of(src_chip * PAIR + core * BLK + first, 16), rows), :]

    def remote(ref, link, sem):
        return pltpu.make_async_remote_copy(
            src_ref=ref, dst_ref=ref, send_sem=send_sem.at[links.index(link)], recv_sem=sem,
            device_id=peers[link], device_id_type=pl.DeviceIdType.MESH,
        )

    def forward(dz, dy, src_chip):
        for first_row, rows, first, way in PIECES:
            for link, go in hops(dz, dy, first, way).items():

                @pl.when(go)
                def _():
                    remote(rows_of(src_chip, c, first_row, rows), link, recv_sem.at[src_chip]).start()

        remote(rows_of(src_chip, c, 0, BLK), "pair", pair_sem.at[src_chip]).start()

    def attend(src_chip, masked):
        base = pl.multiple_of(src_chip * PAIR, PAIR)
        value = kv[pl.ds(base, PAIR), 256:512]
        for k in range(2):
            key = kv[pl.ds(base, PAIR), k * HEAD : (k + 1) * HEAD]
            scores = lax.dot_general(
                q_s[k], key, (((1,), (1,)), ((), ())), preferred_element_type=jnp.float32
            ) * scale
            if masked:
                q_pos = lax.broadcasted_iota(jnp.int32, scores.shape, 0) % BLK + c * BLK
                k_pos = lax.broadcasted_iota(jnp.int32, scores.shape, 1)
                scores = jnp.where(k_pos <= q_pos, scores, FLOOR)
            old = m_s[k]
            new = jnp.maximum(old, jnp.max(scores, axis=1, keepdims=True))
            fade = jnp.exp2(old - new)
            weights = jnp.exp2(scores - jnp.tile(new, (1, PAIR // 128)))
            if masked:
                weights = jnp.where(k_pos <= q_pos, weights, 0.0)
            part = weights[:, 0:128]
            for t in range(1, PAIR // 128):
                part = part + weights[:, t * 128 : (t + 1) * 128]
            m_s[k] = new
            l_s[k] = l_s[k] * fade + part
            acc_s[k] = acc_s[k] * jnp.tile(fade, (1, VD // 128)) + jnp.dot(
                weights.astype(jnp.bfloat16), value, preferred_element_type=jnp.float32
            )

    forward(jnp.int32(0), jnp.int32(0), chip)

    def tell(peer):
        return pltpu.make_async_remote_copy(
            src_ref=cbuf.at[z], dst_ref=cbuf.at[z], send_sem=send_sem.at[5], recv_sem=code_sem,
            device_id=peer, device_id_type=pl.DeviceIdType.MESH,
        )

    for peer in [peers["z+"], peers["z-"]] + far:
        tell(peer).start()

    def all_told():
        ref = cbuf.at[0 : NZ - 1]
        return pltpu.make_async_remote_copy(
            src_ref=ref, dst_ref=ref, send_sem=send_sem.at[5], recv_sem=code_sem,
            device_id=peers["z+"], device_id_type=pl.DeviceIdType.MESH,
        )

    def places(q):
        slot = lax.broadcasted_iota(jnp.int32, (SLOTS, 128), 0).astype(jnp.float32)
        lane = lax.broadcasted_iota(jnp.int32, (SLOTS, 128), 1).astype(jnp.float32)
        expert = jnp.floor((slot + 0.5) * (1.0 / GROUP))
        inside = slot - expert * GROUP
        source = jnp.floor((inside + 0.5) * (1.0 / CAP))
        want = (z * SLAB * CAP).astype(jnp.float32) + expert * CAP + (inside - source * CAP)
        both = cbuf[2 * q] + cbuf[2 * q + 1]
        of_me = source == (2.0 * q.astype(jnp.float32) + jnp.floor(lane * (1.0 / ROWS)))
        weight = jnp.zeros((SLOTS, 128), jnp.float32)
        hit = jnp.zeros((SLOTS, 128), jnp.float32)
        for j in range(TOPK):
            same = of_me & (both[j : j + 1, :] == want)
            hit = hit + jnp.where(same, 1.0, 0.0)
            weight = weight + jnp.where(same, both[TOPK + j : TOPK + j + 1, :], 0.0)
        span = pl.ds(pl.multiple_of(q * 128, 128), 128)
        place_ref[:, span] = hit.astype(jnp.bfloat16)
        turned = weight.T
        high = turned.astype(jnp.bfloat16)
        high_ref[span, :] = high
        low_ref[span, :] = (turned - high.astype(jnp.float32)).astype(jnp.bfloat16)

    dz_table = [o[0] for o in ORDER]
    dy_table = [o[1] for o in ORDER]

    def place(e):
        dz, dy = lookup(dz_table, e), lookup(dy_table, e)
        return dz, dy, ((z - dz + NZ) % NZ) * NY + (y - dy + NY) % NY

    def step(e, carry):
        @pl.when(e < NCHIP)
        def _():
            dz, dy, src = place(e)
            remote(rows_of(src, c, 0, BLK), "z+", recv_sem.at[src]).wait_recv()
            forward(dz, dy, src)

        _, _, last = place(e - 1)
        remote(rows_of(last, 1 - c, 0, BLK), "pair", pair_sem.at[last]).wait_recv()

        @pl.when(e == 1)
        def _():
            attend(chip, True)

        @pl.when(e == 4)
        def _():
            all_told().wait_recv()

        @pl.when((e >= 4) & (e < 20) & (e % 4 == 0))
        def _():
            places((e - 4) // 4)

        @pl.when((e > 1) & (last < chip))
        def _():
            attend(last, False)

        return carry

    lax.fori_loop(1, NCHIP + 1, step, 0)

    head_rows = []
    for k in range(2):
        total = jnp.sum(l_s[k], axis=1, keepdims=True)
        head_rows.append(acc_s[k] / total)
    for h in range(2):
        span = slice(h * BLK, (h + 1) * BLK)
        head = head_rows[0][span] - lam_ref[h] * head_rows[1][span]
        head = head * lax.rsqrt(jnp.mean(head * head, axis=1, keepdims=True) + 1e-05)
        out_ref[:, h * VD : (h + 1) * VD] = head.astype(jnp.bfloat16)

    for link, rows in step_counts().items():
        remote(kv.at[pl.ds(0, rows), :], link, recv_sem.at[0]).wait_send()
    remote(kv.at[pl.ds(0, NCHIP * BLK), :], "pair", recv_sem.at[0]).wait_send()
    all_told().wait_send()


def attention(head_lambda, q_first, q_second, k_first, k_second, values, routes, route_w):
    vmem = pl.BlockSpec(memory_space=pltpu.VMEM)
    hbm = pl.BlockSpec(memory_space=pl.ANY)
    return pl.pallas_call(
        attn_kernel,
        out_shape=[
            jax.ShapeDtypeStruct(shape, jnp.bfloat16)
            for shape in (
                (BLK, 2 * VD), (SLOTS, NZ * ROWS), (NZ * ROWS, SLOTS), (NZ * ROWS, SLOTS)
            )
        ],
        in_specs=[pl.BlockSpec(memory_space=pltpu.SMEM)] + [hbm] * 5 + [vmem] * 2,
        out_specs=[vmem] * 4,
        scratch_shapes=[
            pltpu.VMEM((NCHIP * PAIR, KVW), jnp.bfloat16),
            pltpu.VMEM((2, 2 * BLK, HEAD), jnp.bfloat16),
            pltpu.VMEM((2, 2 * BLK, 128), jnp.float32),
            pltpu.VMEM((2, 2 * BLK, 128), jnp.float32),
            pltpu.VMEM((2, 2 * BLK, VD), jnp.float32),
            pltpu.SemaphoreType.DMA((7,)),
            pltpu.SemaphoreType.DMA((6,)),
            pltpu.SemaphoreType.DMA((NCHIP,)),
            pltpu.SemaphoreType.DMA((NCHIP,)),
            pltpu.VMEM((NZ, 8, 128), jnp.float32),
            pltpu.SemaphoreType.DMA,
        ],
        compiler_params=pltpu.CompilerParams(
            collective_id=0, has_side_effects=True, vmem_limit_bytes=63 * 1024 * 1024
        ),
        name="attend",
    )(head_lambda, q_first, q_second, k_first, k_second, values, routes.T, route_w.T)


D = 4096
ROWS = 64
TP = 4
TOPK = 4
SLAB = 2 * NY
CAP = 6
GROUP = NZ * CAP
SLOTS = SLAB * GROUP
NC = 16
W = D // NC
F = 128
MESH = pl.DeviceIdType.MESH
SUM_LAG, RESID_LAG = 3, 6
HOP_LAGS = tuple(RESID_LAG + n for n in (4, 6, 8))
PACK_LAG, ENTER_LAG = RESID_LAG + 10, RESID_LAG + 14
SHARE_LAG = RESID_LAG + 4
RETURN_LAGS = (3, 5, 8, 11, 14)


def moe_kernel(
    attn_hbm, stream_hbm, gain_hbm, place_hbm, high_hbm, low_hbm,
    w_out_hbm, wg_hbm, wu_hbm, wd_hbm, sg_hbm, su_hbm, sd_hbm,
    out_ref,
    attn_s, stream_s, gain_s, wo, wgu, wd, sgu, sd,
    op_all, op_out, op_in, resid_s, square_s, zbuf, place_s, back_hi, back_lo,
    turn_s, inv_own, inv_z, inv_send, inv_slot, inv_sh,
    ysend, xbuf, hid_s, hb_s, rsend, ret, part_s, rs_out, rs_in,
    sh_all, sh_out, sh_pass, sh_in,
    wo_sem, load_sem, send_sem, op_sem, z_sem, y_sem, r_sem, rs_sem,
    sh_sem, shr_sem, inv_z_sem, inv_slot_sem, inv_sh_sem,
):
    me = lax.axis_index("sp")
    tp = lax.axis_index("tp")
    mine = me % SLAB
    z = me // SLAB
    half = ROWS // 2

    def to_z(step):
        return {"sp": ((z + step + NZ) % NZ) * SLAB + mine}

    def to_slab(step):
        return {"sp": z * SLAB + (mine + step) % SLAB}

    def to_tp(step):
        return {"tp": (tp + step + TP) % TP}

    def remote(src, dst, group, sem, device):
        return pltpu.make_async_remote_copy(
            src_ref=src, dst_ref=dst, send_sem=send_sem.at[group], recv_sem=sem,
            device_id=device, device_id_type=MESH,
        )

    def arrived(ref, sem):
        remote(ref, ref, 0, sem, to_z(1)).wait_recv()

    def left(ref, group):
        remote(ref, ref, group, load_sem.at[0], to_z(1)).wait_send()

    def cols(k):
        return pl.ds(pl.multiple_of(k * W, W), W)

    def rows(first, count):
        return pl.ds(pl.multiple_of(first, 16), count)

    def wo_load(k):
        return pltpu.make_async_copy(w_out_hbm.at[:, cols(k)], wo.at[:, cols(k)], wo_sem.at[k])

    early = [
        pltpu.make_async_copy(attn_hbm, attn_s, load_sem.at[6]),
        pltpu.make_async_copy(stream_hbm, stream_s, load_sem.at[7]),
        pltpu.make_async_copy(gain_hbm, gain_s, load_sem.at[8]),
    ]
    for load in early:
        load.start()
    for k in range(NC):
        wo_load(k).start()
    loads = [
        pltpu.make_async_copy(wg_hbm.at[0], wgu.at[:, 0:F], load_sem.at[0]),
        pltpu.make_async_copy(wu_hbm.at[0], wgu.at[:, F : 2 * F], load_sem.at[1]),
        pltpu.make_async_copy(wd_hbm.at[0], wd, load_sem.at[2]),
        pltpu.make_async_copy(sg_hbm, sgu.at[:, 0:F], load_sem.at[3]),
        pltpu.make_async_copy(su_hbm, sgu.at[:, F : 2 * F], load_sem.at[4]),
        pltpu.make_async_copy(sd_hbm, sd, load_sem.at[5]),
        pltpu.make_async_copy(place_hbm, place_s, load_sem.at[9]),
        pltpu.make_async_copy(high_hbm, back_hi, load_sem.at[10]),
        pltpu.make_async_copy(low_hbm, back_lo, load_sem.at[11]),
    ]
    for load in loads:
        load.start()

    barrier = pltpu.get_barrier_semaphore()
    peers = [to_z(s) for s in range(1, NZ)] + [to_slab(s) for s in range(1, SLAB)]
    peers += [to_tp(s) for s in range(1, TP)]
    for peer in peers:
        pl.semaphore_signal(barrier, inc=1, device_id=peer, device_id_type=MESH)

    turn_s[...] = jnp.zeros_like(turn_s)
    square_s[...] = jnp.zeros_like(square_s)
    hid_s[...] = jnp.zeros_like(hid_s)

    pl.semaphore_wait(barrier, len(peers))
    for load in early:
        load.wait()

    def ring_out(d, stage, first, count, k, src, group, landing, sem):
        dst = landing.at[d, k, stage, first : first + count, :]
        remote(src, dst, group, sem.at[d, k, stage], to_tp(1 - 2 * d)).start()

    def ring_first(k, table_ref, landing, group, sem):
        for d in range(2):
            src = table_ref.at[k, rows(((tp + 2) % TP) * ROWS + d * half, half), :]
            ring_out(d, 0, d * half, half, k, src, group, landing, sem)

    def ring_second(k, table_ref, passing, landing, group, sem):
        for d in range(2):
            first, other = d * half, (1 - d) * half
            owner = (tp + 1 - 2 * d + TP) % TP
            arrived(landing.at[d, k, 0, first : first + half, :], sem.at[d, k, 0])
            piece = table_ref[k, rows(owner * ROWS + first, half), :].astype(jnp.float32)
            piece = piece + landing[d, k, 0, first : first + half, :].astype(jnp.float32)
            passing[d, k, first : first + half, :] = piece.astype(jnp.bfloat16)
            passing[d, k, other : other + half, :] = table_ref[k, rows(owner * ROWS + other, half), :]
            ring_out(d, 1, 0, ROWS, k, passing.at[d, k], group, landing, sem)

    def ring_total(k, table_ref, landing, sem):
        total = table_ref[k, rows(tp * ROWS, ROWS), :].astype(jnp.float32)
        for d in range(2):
            arrived(landing.at[d, k, 1], sem.at[d, k, 1])
            total = total + landing[d, k, 1].astype(jnp.float32)
        return total

    def project(k):
        wo_load(k).wait()
        op_all[k] = jnp.dot(
            attn_s[...], wo[:, cols(k)], preferred_element_type=jnp.float32
        ).astype(jnp.bfloat16)
        ring_first(k, op_all, op_in, 1, op_sem)

    def pass_rows(k, owner, first, count, way):
        ref = zbuf.at[k, rows(owner * ROWS + first, count), :]
        remote(ref, ref, 3, z_sem.at[k, owner], to_z(way)).start()

    def share_rows(k, owner, first, count, way):
        ref = sh_all.at[k, rows(owner * ROWS + first, count), :]
        remote(ref, ref, 2, sh_sem.at[k, owner], to_tp(way)).start()

    def residual(k):
        total = ring_total(k, op_all, op_in, op_sem)
        resid = (stream_s[:, cols(k)].astype(jnp.float32) + total).astype(jnp.bfloat16)
        resid_s[k] = resid
        wide = resid.astype(jnp.float32)
        gain = jnp.concatenate(
            [gain_s[pl.ds(k * (W // 128) + t, 1), :] for t in range(W // 128)], axis=1
        )
        scaled = (wide * gain).astype(jnp.bfloat16)
        zbuf[k, rows(z * ROWS, ROWS), :] = scaled
        sh_all[k, rows(tp * ROWS, ROWS), :] = scaled
        for way in (1, -1):
            pass_rows(k, z, 0, ROWS, way)
            share_rows(k, tp, 0, ROWS, way)
        wide = wide * wide
        square = square_s[...]
        for t in range(W // 128):
            square = square + wide[:, t * 128 : (t + 1) * 128]
        square_s[...] = square

    def send_inverse():
        mean = jnp.sum(square_s[...], axis=1, keepdims=True) * (1.0 / D)
        inverse = jnp.broadcast_to(lax.rsqrt(mean + 1e-06), (ROWS, 128))
        inv_sh[rows(tp * ROWS, ROWS), :] = inverse
        turn_s[rows((z % 2) * ROWS, ROWS), :] = inverse
        inv_own[...] = turn_s[...].T[0:8, :]
        inv_z[z] = inv_own[...]
        for s in range(1, NZ):
            remote(inv_own, inv_z.at[z], 8, inv_z_sem, to_z(s)).start()
        own = inv_sh.at[rows(tp * ROWS, ROWS), :]
        for r in range(1, TP):
            remote(own, own, 9, inv_sh_sem, to_tp(r)).start()

    def spread_inverse():
        arrived(inv_z.at[0 : NZ - 1], inv_z_sem)
        total = jnp.zeros((SLOTS, 128), jnp.float32)
        for q in range(NZ // 2):
            both = inv_z[2 * q] + inv_z[2 * q + 1]
            total = total + place_s[:, q * 128 : (q + 1) * 128].astype(jnp.float32) * both[0:1, :]
        inv_send[...] = jnp.broadcast_to(jnp.sum(total, axis=1, keepdims=True), (SLOTS, 128))
        land = inv_slot.at[rows(mine * GROUP, GROUP), :]
        for s in range(1, SLAB):
            src = inv_send.at[rows(((mine + s) % SLAB) * GROUP, GROUP), :]
            remote(src, land, 10, inv_slot_sem, to_slab(s)).start()
        inv_slot[rows(mine * GROUP, GROUP), :] = inv_send[rows(mine * GROUP, GROUP), :]

    def relay(k, step):
        below, above = (z - step + NZ) % NZ, (z + step) % NZ
        arrived(zbuf.at[k, rows(below * ROWS, ROWS), :], z_sem.at[k, below])
        pass_rows(k, below, 0, ROWS if step < 3 else half, 1)
        arrived(zbuf.at[k, rows(above * ROWS, ROWS), :], z_sem.at[k, above])
        if step < 3:
            pass_rows(k, above, 0, ROWS, -1)
        else:
            pass_rows(k, above, half, half, -1)

    def share(k):
        below, above = (tp + TP - 1) % TP, (tp + 1) % TP
        arrived(sh_all.at[k, rows(below * ROWS, ROWS), :], sh_sem.at[k, below])
        share_rows(k, below, 0, half, 1)
        arrived(sh_all.at[k, rows(above * ROWS, ROWS), :], sh_sem.at[k, above])
        share_rows(k, above, half, half, -1)

    def spread(store, landing, k, sem, group):
        for s in (2, 6, 1, 3, 5, 7, 4):
            src = store.at[k, rows(((mine + s) % SLAB) * GROUP, GROUP), :]
            dst = landing.at[k, rows(mine * GROUP, GROUP), :]
            remote(src, dst, group, sem.at[k], to_slab(s)).start()
        landing[k, rows(mine * GROUP, GROUP), :] = store[k, rows(mine * GROUP, GROUP), :]

    def pack(k):
        far = (z + 4) % NZ
        arrived(zbuf.at[k, rows(far * ROWS, ROWS), :], z_sem.at[k, far])
        ysend[k] = jnp.dot(
            place_s[...], zbuf[k], preferred_element_type=jnp.float32
        ).astype(jnp.bfloat16)
        spread(ysend, xbuf, k, y_sem, 4)

    def enter(k):
        arrived(xbuf.at[k, 0 : SLOTS - GROUP, :], y_sem.at[k])
        hid_s[...] += jnp.dot(xbuf[k], wgu[cols(k), :], preferred_element_type=jnp.float32)

    def gated(sums, inverse):
        g = sums[:, 0:F] * inverse
        return (g / (1.0 + jnp.exp(-g)) * (sums[:, F : 2 * F] * inverse)).astype(jnp.bfloat16)

    def shared():
        def gate(k, acc):
            far = (tp + 2) % TP
            arrived(sh_all.at[k, rows(far * ROWS, ROWS), :], sh_sem.at[k, far])
            return acc + jnp.dot(sh_all[k], sgu[cols(k), :], preferred_element_type=jnp.float32)

        acc = lax.fori_loop(0, NC, gate, jnp.zeros((TP * ROWS, 2 * F), jnp.float32))
        arrived(inv_sh.at[0 : (TP - 1) * ROWS, :], inv_sh_sem)
        hidden = gated(acc, inv_sh[...])

        def down(k, carry):
            sh_out[k] = jnp.dot(
                hidden, sd[:, cols(k)], preferred_element_type=jnp.float32
            ).astype(jnp.bfloat16)
            ring_first(k, sh_out, sh_in, 5, shr_sem)
            return carry

        lax.fori_loop(0, NC, down, 0)

    def guarded(k, action):
        @pl.when((k >= 0) & (k < NC))
        def _():
            action(k)

    def way_out(t, carry):
        guarded(t, project)

        @pl.when(t == RESID_LAG + 2)
        def _():
            for load in loads:
                load.wait()

        guarded(t - SUM_LAG, lambda k: ring_second(k, op_all, op_out, op_in, 1, op_sem))
        for step in (1, 2, 3):
            guarded(t - HOP_LAGS[step - 1], lambda k, step=step: relay(k, step))
        guarded(t - RESID_LAG, residual)

        @pl.when(t == NC - 1 + RESID_LAG)
        def _():
            send_inverse()

        guarded(t - SHARE_LAG, share)
        guarded(t - PACK_LAG, pack)
        guarded(t - ENTER_LAG, enter)

        @pl.when(t == NC + ENTER_LAG - 4)
        def _():
            spread_inverse()

        @pl.when(t == NC + 2 + SHARE_LAG)
        def _():
            shared()

        return carry

    lax.fori_loop(0, NC + ENTER_LAG, way_out, 0)

    arrived(inv_slot.at[0 : SLOTS - GROUP, :], inv_slot_sem)
    hb_s[...] = gated(hid_s[...], inv_slot[...])

    def leave(k):
        rsend[k] = jnp.dot(
            hb_s[...], wd[:, cols(k)], preferred_element_type=jnp.float32
        ).astype(jnp.bfloat16)
        spread(rsend, ret, k, r_sem, 6)

    def hand_on(d, k, stage, first, count):
        src = rs_out.at[d, k, stage, first : first + count, :]
        dst = rs_in.at[d, k, stage, first : first + count, :]
        remote(src, dst, 7, rs_sem.at[d, k, stage], to_z(1 - 2 * d)).start()

    def combine(k):
        arrived(ret.at[k, 0 : SLOTS - GROUP, :], r_sem.at[k])
        part_s[k] = jnp.dot(
            back_hi[...], ret[k], preferred_element_type=jnp.float32
        ) + jnp.dot(back_lo[...], ret[k], preferred_element_type=jnp.float32)
        owner = (z + 4) % NZ
        for d in range(2):
            piece = part_s[k, rows(owner * ROWS + d * half, half), :]
            rs_out[d, k, 0, d * half : (d + 1) * half, :] = piece.astype(jnp.bfloat16)
            hand_on(d, k, 0, d * half, half)

    def add_on(k, stage):
        for d in range(2):
            owner = (z + (1 - 2 * d) * (4 - stage) + NZ) % NZ
            first = d * half if stage == 1 else 0
            count = half if stage == 1 else ROWS
            arrived(rs_in.at[d, k, stage - 1, first : first + count, :], rs_sem.at[d, k, stage - 1])
            piece = part_s[k, rows(owner * ROWS + first, count), :]
            piece = piece + rs_in[d, k, stage - 1, first : first + count, :].astype(jnp.float32)
            rs_out[d, k, stage, first : first + count, :] = piece.astype(jnp.bfloat16)
            if stage == 1:
                other = (1 - d) * half
                piece = part_s[k, rows(owner * ROWS + other, half), :]
                rs_out[d, k, stage, other : other + half, :] = piece.astype(jnp.bfloat16)
            hand_on(d, k, stage, 0, ROWS)

    def finish(k):
        total = part_s[k, rows(z * ROWS, ROWS), :]
        for d in range(2):
            arrived(rs_in.at[d, k, 3], rs_sem.at[d, k, 3])
            total = total + rs_in[d, k, 3].astype(jnp.float32)
        total = total + ring_total(k, sh_out, sh_in, shr_sem)
        out_ref[:, cols(k)] = (resid_s[k].astype(jnp.float32) + total).astype(jnp.bfloat16)

    b1, b2, b3, b4, b5 = RETURN_LAGS

    def give_back(t, carry):
        guarded(t, leave)
        guarded(t - b4, lambda k: add_on(k, 3))
        guarded(t - b3, lambda k: add_on(k, 2))
        guarded(t - b2, lambda k: add_on(k, 1))
        guarded(t - b1, combine)
        guarded(t - b1, lambda k: ring_second(k, sh_out, sh_pass, sh_in, 5, shr_sem))
        guarded(t - b5, finish)
        return carry

    lax.fori_loop(0, NC + b5, give_back, 0)

    left(sh_all.at[:, 0 : 3 * ROWS, :], 1)
    left(sh_all.at[:, 0 : 3 * ROWS, :], 2)
    left(zbuf.at[:, 0 : 7 * ROWS, :], 3)
    left(xbuf.at[:, 0 : SLOTS - GROUP, :], 4)
    left(sh_all.at[:, 0 : 3 * ROWS, :], 5)
    left(ret.at[:, 0 : SLOTS - GROUP, :], 6)
    left(zbuf.at[:, 0 : 7 * ROWS, :], 7)
    left(inv_z.at[0 : NZ - 1], 8)
    left(inv_sh.at[0 : (TP - 1) * ROWS, :], 9)
    left(inv_slot.at[0 : SLOTS - GROUP, :], 10)


def moe(
    attn_rows, stream_in, norm_gain, places, w_out, w_gate, w_up, w_down, s_gate, s_up, s_down
):
    vmem = pl.BlockSpec(memory_space=pltpu.VMEM)
    hbm = pl.BlockSpec(memory_space=pl.ANY)
    bf, f32 = jnp.bfloat16, jnp.float32
    dma = pltpu.SemaphoreType.DMA
    return pl.pallas_call(
        moe_kernel,
        out_shape=jax.ShapeDtypeStruct((ROWS, D), bf),
        in_specs=[hbm] * 13,
        out_specs=vmem,
        scratch_shapes=[
            pltpu.VMEM((TP * ROWS, 2 * VD), bf),
            pltpu.VMEM((ROWS, D), bf),
            pltpu.VMEM((D // 128, 128), f32),
            pltpu.VMEM((2 * VD, D), bf),
            pltpu.VMEM((D, 2 * F), bf),
            pltpu.VMEM((F, D), bf),
            pltpu.VMEM((D, 2 * F), bf),
            pltpu.VMEM((F, D), bf),
            pltpu.VMEM((NC, TP * ROWS, W), bf),
            pltpu.VMEM((2, NC, ROWS, W), bf),
            pltpu.VMEM((2, NC, 2, ROWS, W), bf),
            pltpu.VMEM((NC, ROWS, W), bf),
            pltpu.VMEM((ROWS, 128), f32),
            pltpu.VMEM((NC, NZ * ROWS, W), bf),
            pltpu.VMEM((SLOTS, NZ * ROWS), bf),
            pltpu.VMEM((NZ * ROWS, SLOTS), bf),
            pltpu.VMEM((NZ * ROWS, SLOTS), bf),
            pltpu.VMEM((2 * ROWS, 128), f32),
            pltpu.VMEM((8, 128), f32),
            pltpu.VMEM((NZ, 8, 128), f32),
            pltpu.VMEM((SLOTS, 128), f32),
            pltpu.VMEM((SLOTS, 128), f32),
            pltpu.VMEM((TP * ROWS, 128), f32),
            pltpu.VMEM((NC, SLOTS, W), bf),
            pltpu.VMEM((NC, SLOTS, W), bf),
            pltpu.VMEM((SLOTS, 2 * F), f32),
            pltpu.VMEM((SLOTS, F), bf),
            pltpu.VMEM((NC, SLOTS, W), bf),
            pltpu.VMEM((NC, SLOTS, W), bf),
            pltpu.VMEM((NC, NZ * ROWS, W), f32),
            pltpu.VMEM((2, NC, 4, ROWS, W), bf),
            pltpu.VMEM((2, NC, 4, ROWS, W), bf),
            pltpu.VMEM((NC, TP * ROWS, W), bf),
            pltpu.VMEM((NC, TP * ROWS, W), bf),
            pltpu.VMEM((2, NC, ROWS, W), bf),
            pltpu.VMEM((2, NC, 2, ROWS, W), bf),
            dma((NC,)),
            dma((12,)),
            dma((11,)),
            dma((2, NC, 2)),
            dma((NC, NZ)),
            dma((NC,)),
            dma((NC,)),
            dma((2, NC, 4)),
            dma((NC, TP)),
            dma((2, NC, 2)),
            dma,
            dma,
            dma,
        ],
        compiler_params=pltpu.CompilerParams(
            collective_id=1, has_side_effects=True, vmem_limit_bytes=67043328
        ),
        name="experts",
    )(
        attn_rows, stream_in, norm_gain.reshape(D // 128, 128), *places,
        w_out, w_gate, w_up, w_down, s_gate, s_up, s_down,
    )


def local(
    stream_in,
    q_first,
    q_second,
    k_first,
    k_second,
    values,
    head_lambda,
    w_out,
    norm_gain,
    routes,
    route_w,
    w_gate,
    w_up,
    w_down,
    s_gate,
    s_up,
    s_down,
):
    attn_rows, *places = attention(
        head_lambda, q_first, q_second, k_first, k_second, values, routes, route_w
    )
    return moe(
        attn_rows, stream_in, norm_gain, places, w_out, w_gate, w_up, w_down, s_gate, s_up, s_down
    )


def solution(mesh):
    return jax.shard_map(
        local,
        mesh=mesh,
        in_specs=(
            P(("sp", "tp"), None),
            P("sp", "tp"),
            P("sp", "tp"),
            P("sp", "tp"),
            P("sp", "tp"),
            P("sp", "tp"),
            P("tp"),
            P("tp", None),
            P(),
            P(("sp", "tp"), None),
            P(("sp", "tp"), None),
            P("sp", None, None),
            P("sp", None, None),
            P("sp", None, None),
            P(None, "tp"),
            P(None, "tp"),
            P("tp", None),
        ),
        out_specs=P(("sp", "tp"), None),
        check_vma=False,
    )
```

```python
import jax
import jax.numpy as jnp
from jax import lax
from jax.experimental import pallas as pl
from jax.experimental.pallas import tpu as pltpu
from jax.sharding import PartitionSpec as P

HEAD = 128
VD = 256
FLOOR = -1e30
NZ = 8
NY = 4
NCHIP = NZ * NY
BLK = 256
PAIR = 2 * BLK
KVW = 512
LOG2E = 1.4426950408889634

ORDER = sorted(
    [(dz, dy) for dz in (0, 1, -1, 2, -2, 3, -3, 4) for dy in (0, 1, -1, 2)],
    key=lambda a: (abs(a[0]) + abs(a[1]), -abs(a[0]), a),
)
PIECES = ((0, 80, "z", 1), (80, 80, "z", -1), (160, 48, "y", 1), (208, 48, "y", -1))


def step_counts():
    sent = {"z+": 0, "z-": 0, "y+": 0, "y-": 0}
    for dz, dy in ORDER:
        for _, rows, first, way in PIECES:
            for link, go in hops(dz, dy, first, way).items():
                if go:
                    sent[link] += rows
    return sent


def hops(dz, dy, first, way):
    zup = (dz >= 0) & (dz < (4 if way > 0 else 3))
    zdown = (dz <= 0) & (dz > (-3 if way > 0 else -4))
    yup = (dy >= 0) & (dy < (2 if way > 0 else 1))
    ydown = (dy <= 0) & (dy > (-1 if way > 0 else -2))
    if first == "z":
        zup, zdown = zup & (dy == 0), zdown & (dy == 0)
    else:
        yup, ydown = yup & (dz == 0), ydown & (dz == 0)
    return {"z+": zup, "z-": zdown, "y+": yup, "y-": ydown}


def lookup(values, index):
    out = jnp.int32(values[0])
    for k, v in enumerate(values[1:], 1):
        out = jnp.where(index == k, jnp.int32(v), out)
    return out


def attn_kernel(
    lam_ref, q1_hbm, q2_hbm, k1_hbm, k2_hbm, v_hbm, routes_ref, route_w_ref,
    out_ref, place_ref, high_ref, low_ref,
    kv, q_s, m_s, l_s, acc_s, load_sem, send_sem, recv_sem, pair_sem, cbuf, code_sem,
):
    me = lax.axis_index("sp")
    c = me % 2
    y = (me // 2) % NY
    z = me // (2 * NY)
    chip = z * NY + y

    def at(zz, yy, cc):
        return {"sp": ((zz + NZ) % NZ) * (2 * NY) + ((yy + NY) % NY) * 2 + cc}

    peers = {
        "z+": at(z + 1, y, c), "z-": at(z - 1, y, c),
        "y+": at(z, y + 1, c), "y-": at(z, y - 1, c),
        "pair": at(z, y, 1 - c),
    }
    links = ("z+", "z-", "y+", "y-", "pair")
    far = [at(z + step, y, c) for step in range(2, NZ - 1)]

    own = pl.multiple_of(chip * PAIR + c * BLK, BLK)
    loads = []
    for k, (src, lo, hi) in enumerate(((k1_hbm, 0, 128), (k2_hbm, 128, 256), (v_hbm, 256, 512))):
        loads.append(pltpu.make_async_copy(src, kv.at[pl.ds(own, BLK), lo:hi], load_sem.at[k]))
        loads[-1].start()

    for k, ref in enumerate((q1_hbm, q2_hbm)):
        for h in range(2):
            loads.append(
                pltpu.make_async_copy(
                    ref.at[:, h * HEAD : (h + 1) * HEAD],
                    q_s.at[k, h * BLK : (h + 1) * BLK, :],
                    load_sem.at[3 + 2 * k + h],
                )
            )
            loads[-1].start()

    barrier = pltpu.get_barrier_semaphore()
    for link in links:
        pl.semaphore_signal(barrier, inc=1, device_id=peers[link], device_id_type=pl.DeviceIdType.MESH)
    for peer in far:
        pl.semaphore_signal(barrier, inc=1, device_id=peer, device_id_type=pl.DeviceIdType.MESH)

    scale = HEAD ** (-0.5) * LOG2E
    m_s[...] = jnp.full_like(m_s, FLOOR)
    l_s[...] = jnp.zeros_like(l_s)
    acc_s[...] = jnp.zeros_like(acc_s)

    names = lax.broadcasted_iota(jnp.int32, (NZ * SLAB, ROWS), 0)
    hits = jnp.zeros((NZ * SLAB, ROWS), jnp.float32)
    for j in range(TOPK):
        hits = hits + jnp.where(routes_ref[j : j + 1, :] == names, 1.0, 0.0)
    upper = (
        lax.broadcasted_iota(jnp.int32, (ROWS, ROWS), 0)
        < lax.broadcasted_iota(jnp.int32, (ROWS, ROWS), 1)
    )
    before = jnp.dot(
        hits.astype(jnp.bfloat16),
        jnp.where(upper, 1.0, 0.0).astype(jnp.bfloat16),
        preferred_element_type=jnp.float32,
    )
    table = []
    for j in range(TOPK):
        chosen = routes_ref[j : j + 1, :]
        taken = jnp.sum(jnp.where(chosen == names, before, 0.0), axis=0, keepdims=True)
        table.append(chosen.astype(jnp.float32) * CAP + taken)
    for j in range(TOPK):
        table.append(route_w_ref[j : j + 1, :])
    table = jnp.concatenate(table, axis=0)
    odd = (z % 2).astype(jnp.float32)
    cbuf[z] = jnp.concatenate([table * (1.0 - odd), table * odd], axis=1)

    pl.semaphore_wait(barrier, len(links) + len(far))
    for copy in loads:
        copy.wait()

    def rows_of(src_chip, core, first, rows):
        return kv.at[pl.ds(pl.multiple_of(src_chip * PAIR + core * BLK + first, 16), rows), :]

    def remote(ref, link, sem):
        return pltpu.make_async_remote_copy(
            src_ref=ref, dst_ref=ref, send_sem=send_sem.at[links.index(link)], recv_sem=sem,
            device_id=peers[link], device_id_type=pl.DeviceIdType.MESH,
        )

    def forward(dz, dy, src_chip):
        for first_row, rows, first, way in PIECES:
            for link, go in hops(dz, dy, first, way).items():

                @pl.when(go)
                def _():
                    remote(rows_of(src_chip, c, first_row, rows), link, recv_sem.at[src_chip]).start()

        remote(rows_of(src_chip, c, 0, BLK), "pair", pair_sem.at[src_chip]).start()

    def attend(src_chip, masked):
        base = pl.multiple_of(src_chip * PAIR, PAIR)
        value = kv[pl.ds(base, PAIR), 256:512]
        scores, olds = [], []
        for k in range(2):
            key = kv[pl.ds(base, PAIR), k * HEAD : (k + 1) * HEAD]
            scores.append(lax.dot_general(
                q_s[k], key, (((1,), (1,)), ((), ())), preferred_element_type=jnp.float32
            ) * scale)
            olds.append(m_s[k])
        fades, packs = [], []
        for k in range(2):
            score = scores[k]
            if masked:
                q_pos = lax.broadcasted_iota(jnp.int32, score.shape, 0) % BLK + c * BLK
                k_pos = lax.broadcasted_iota(jnp.int32, score.shape, 1)
                score = jnp.where(k_pos <= q_pos, score, FLOOR)
            new = jnp.maximum(olds[k], jnp.max(score, axis=1, keepdims=True))
            fade = jnp.exp2(olds[k] - new)
            weights = jnp.exp2(score - jnp.tile(new, (1, PAIR // 128)))
            if masked:
                weights = jnp.where(k_pos <= q_pos, weights, 0.0)
            part = weights[:, 0:128]
            for t in range(1, PAIR // 128):
                part = part + weights[:, t * 128 : (t + 1) * 128]
            m_s[k] = new
            l_s[k] = l_s[k] * fade + part
            fades.append(fade)
            packs.append(weights.astype(jnp.bfloat16))
        for k in range(2):
            acc_s[k] = acc_s[k] * jnp.tile(fades[k], (1, VD // 128)) + jnp.dot(
                packs[k], value, preferred_element_type=jnp.float32
            )

    forward(jnp.int32(0), jnp.int32(0), chip)

    def tell(peer):
        return pltpu.make_async_remote_copy(
            src_ref=cbuf.at[z], dst_ref=cbuf.at[z], send_sem=send_sem.at[5], recv_sem=code_sem,
            device_id=peer, device_id_type=pl.DeviceIdType.MESH,
        )

    for peer in [peers["z+"], peers["z-"]] + far:
        tell(peer).start()

    def all_told():
        ref = cbuf.at[0 : NZ - 1]
        return pltpu.make_async_remote_copy(
            src_ref=ref, dst_ref=ref, send_sem=send_sem.at[5], recv_sem=code_sem,
            device_id=peers["z+"], device_id_type=pl.DeviceIdType.MESH,
        )

    def places(q):
        slot = lax.broadcasted_iota(jnp.int32, (SLOTS, 128), 0).astype(jnp.float32)
        lane = lax.broadcasted_iota(jnp.int32, (SLOTS, 128), 1).astype(jnp.float32)
        expert = jnp.floor((slot + 0.5) * (1.0 / GROUP))
        inside = slot - expert * GROUP
        source = jnp.floor((inside + 0.5) * (1.0 / CAP))
        want = (z * SLAB * CAP).astype(jnp.float32) + expert * CAP + (inside - source * CAP)
        both = cbuf[2 * q] + cbuf[2 * q + 1]
        of_me = source == (2.0 * q.astype(jnp.float32) + jnp.floor(lane * (1.0 / ROWS)))
        weight = jnp.zeros((SLOTS, 128), jnp.float32)
        hit = jnp.zeros((SLOTS, 128), jnp.float32)
        for j in range(TOPK):
            same = of_me & (both[j : j + 1, :] == want)
            hit = hit + jnp.where(same, 1.0, 0.0)
            weight = weight + jnp.where(same, both[TOPK + j : TOPK + j + 1, :], 0.0)
        span = pl.ds(pl.multiple_of(q * 128, 128), 128)
        place_ref[:, span] = hit.astype(jnp.bfloat16)
        turned = weight.T
        high = turned.astype(jnp.bfloat16)
        high_ref[span, :] = high
        low_ref[span, :] = (turned - high.astype(jnp.float32)).astype(jnp.bfloat16)

    dz_table = [o[0] for o in ORDER]
    dy_table = [o[1] for o in ORDER]

    def place(e):
        dz, dy = lookup(dz_table, e), lookup(dy_table, e)
        return dz, dy, ((z - dz + NZ) % NZ) * NY + (y - dy + NY) % NY

    def step(e, carry):
        @pl.when(e < NCHIP)
        def _():
            dz, dy, src = place(e)
            remote(rows_of(src, c, 0, BLK), "z+", recv_sem.at[src]).wait_recv()
            forward(dz, dy, src)

        _, _, last = place(e - 1)
        remote(rows_of(last, 1 - c, 0, BLK), "pair", pair_sem.at[last]).wait_recv()

        @pl.when(e == 1)
        def _():
            attend(chip, True)

        @pl.when(e == 4)
        def _():
            all_told().wait_recv()

        @pl.when((e >= 4) & (e < 20) & (e % 4 == 0))
        def _():
            places((e - 4) // 4)

        @pl.when((e > 1) & (last < chip))
        def _():
            attend(last, False)

        return carry

    lax.fori_loop(1, NCHIP + 1, step, 0)

    head_rows = []
    for k in range(2):
        total = jnp.sum(l_s[k], axis=1, keepdims=True)
        head_rows.append(acc_s[k] / total)
    for h in range(2):
        span = slice(h * BLK, (h + 1) * BLK)
        head = head_rows[0][span] - lam_ref[h] * head_rows[1][span]
        head = head * lax.rsqrt(jnp.mean(head * head, axis=1, keepdims=True) + 1e-05)
        out_ref[:, h * VD : (h + 1) * VD] = head.astype(jnp.bfloat16)

    for link, rows in step_counts().items():
        remote(kv.at[pl.ds(0, rows), :], link, recv_sem.at[0]).wait_send()
    remote(kv.at[pl.ds(0, NCHIP * BLK), :], "pair", recv_sem.at[0]).wait_send()
    all_told().wait_send()


def attention(head_lambda, q_first, q_second, k_first, k_second, values, routes, route_w):
    vmem = pl.BlockSpec(memory_space=pltpu.VMEM)
    hbm = pl.BlockSpec(memory_space=pl.ANY)
    return pl.pallas_call(
        attn_kernel,
        out_shape=[
            jax.ShapeDtypeStruct(shape, jnp.bfloat16)
            for shape in (
                (BLK, 2 * VD), (SLOTS, NZ * ROWS), (NZ * ROWS, SLOTS), (NZ * ROWS, SLOTS)
            )
        ],
        in_specs=[pl.BlockSpec(memory_space=pltpu.SMEM)] + [hbm] * 5 + [vmem] * 2,
        out_specs=[vmem] * 4,
        scratch_shapes=[
            pltpu.VMEM((NCHIP * PAIR, KVW), jnp.bfloat16),
            pltpu.VMEM((2, 2 * BLK, HEAD), jnp.bfloat16),
            pltpu.VMEM((2, 2 * BLK, 128), jnp.float32),
            pltpu.VMEM((2, 2 * BLK, 128), jnp.float32),
            pltpu.VMEM((2, 2 * BLK, VD), jnp.float32),
            pltpu.SemaphoreType.DMA((7,)),
            pltpu.SemaphoreType.DMA((6,)),
            pltpu.SemaphoreType.DMA((NCHIP,)),
            pltpu.SemaphoreType.DMA((NCHIP,)),
            pltpu.VMEM((NZ, 8, 128), jnp.float32),
            pltpu.SemaphoreType.DMA,
        ],
        compiler_params=pltpu.CompilerParams(
            collective_id=0, has_side_effects=True, vmem_limit_bytes=63 * 1024 * 1024
        ),
        name="attend",
    )(head_lambda, q_first, q_second, k_first, k_second, values, routes.T, route_w.T)


D = 4096
ROWS = 64
TP = 4
TOPK = 4
SLAB = 2 * NY
CAP = 6
GROUP = NZ * CAP
SLOTS = SLAB * GROUP
NC = 16
W = D // NC
F = 128
MESH = pl.DeviceIdType.MESH
SUM_LAG, RESID_LAG = 3, 6
HOP_LAGS = tuple(RESID_LAG + n for n in (4, 6, 8))
PACK_LAG, ENTER_LAG = RESID_LAG + 10, RESID_LAG + 14
SHARE_LAG = RESID_LAG + 4
RETURN_LAGS = (3, 5, 8, 11, 14)


def moe_kernel(
    attn_hbm, stream_hbm, gain_hbm, place_hbm, high_hbm, low_hbm,
    w_out_hbm, wg_hbm, wu_hbm, wd_hbm, sg_hbm, su_hbm, sd_hbm,
    out_ref,
    attn_s, stream_s, gain_s, wo, wgu, wd, sgu, sd,
    op_all, op_out, op_in, resid_s, square_s, zbuf, place_s, back_hi, back_lo,
    turn_s, inv_own, inv_z, inv_send, inv_slot, inv_sh,
    ysend, xbuf, hid_s, hb_s, rsend, ret, part_s, rs_out, rs_in,
    sh_all, sh_out, sh_pass, sh_in,
    wo_sem, load_sem, send_sem, op_sem, z_sem, y_sem, r_sem, rs_sem,
    sh_sem, shr_sem, inv_z_sem, inv_slot_sem, inv_sh_sem,
):
    me = lax.axis_index("sp")
    tp = lax.axis_index("tp")
    mine = me % SLAB
    z = me // SLAB
    half = ROWS // 2

    def to_z(step):
        return {"sp": ((z + step + NZ) % NZ) * SLAB + mine}

    def to_slab(step):
        return {"sp": z * SLAB + (mine + step) % SLAB}

    def to_tp(step):
        return {"tp": (tp + step + TP) % TP}

    def remote(src, dst, group, sem, device):
        return pltpu.make_async_remote_copy(
            src_ref=src, dst_ref=dst, send_sem=send_sem.at[group], recv_sem=sem,
            device_id=device, device_id_type=MESH,
        )

    def arrived(ref, sem):
        remote(ref, ref, 0, sem, to_z(1)).wait_recv()

    def left(ref, group):
        remote(ref, ref, group, load_sem.at[0], to_z(1)).wait_send()

    def cols(k):
        return pl.ds(pl.multiple_of(k * W, W), W)

    def rows(first, count):
        return pl.ds(pl.multiple_of(first, 16), count)

    def wo_load(k):
        return pltpu.make_async_copy(w_out_hbm.at[:, cols(k)], wo.at[:, cols(k)], wo_sem.at[k])

    early = [
        pltpu.make_async_copy(attn_hbm, attn_s, load_sem.at[6]),
        pltpu.make_async_copy(stream_hbm, stream_s, load_sem.at[7]),
        pltpu.make_async_copy(gain_hbm, gain_s, load_sem.at[8]),
    ]
    for load in early:
        load.start()
    for k in range(NC):
        wo_load(k).start()
    loads = [
        pltpu.make_async_copy(wg_hbm.at[0], wgu.at[:, 0:F], load_sem.at[0]),
        pltpu.make_async_copy(wu_hbm.at[0], wgu.at[:, F : 2 * F], load_sem.at[1]),
        pltpu.make_async_copy(wd_hbm.at[0], wd, load_sem.at[2]),
        pltpu.make_async_copy(sg_hbm, sgu.at[:, 0:F], load_sem.at[3]),
        pltpu.make_async_copy(su_hbm, sgu.at[:, F : 2 * F], load_sem.at[4]),
        pltpu.make_async_copy(sd_hbm, sd, load_sem.at[5]),
        pltpu.make_async_copy(place_hbm, place_s, load_sem.at[9]),
        pltpu.make_async_copy(high_hbm, back_hi, load_sem.at[10]),
        pltpu.make_async_copy(low_hbm, back_lo, load_sem.at[11]),
    ]
    for load in loads:
        load.start()

    barrier = pltpu.get_barrier_semaphore()
    peers = [to_z(s) for s in range(1, NZ)] + [to_slab(s) for s in range(1, SLAB)]
    peers += [to_tp(s) for s in range(1, TP)]
    for peer in peers:
        pl.semaphore_signal(barrier, inc=1, device_id=peer, device_id_type=MESH)

    turn_s[...] = jnp.zeros_like(turn_s)
    square_s[...] = jnp.zeros_like(square_s)
    hid_s[...] = jnp.zeros_like(hid_s)

    pl.semaphore_wait(barrier, len(peers))
    for load in early:
        load.wait()

    def ring_out(d, stage, first, count, k, src, group, landing, sem):
        dst = landing.at[d, k, stage, first : first + count, :]
        remote(src, dst, group, sem.at[d, k, stage], to_tp(1 - 2 * d)).start()

    def ring_first(k, table_ref, landing, group, sem):
        for d in range(2):
            src = table_ref.at[k, rows(((tp + 2) % TP) * ROWS + d * half, half), :]
            ring_out(d, 0, d * half, half, k, src, group, landing, sem)

    def ring_second(k, table_ref, passing, landing, group, sem):
        for d in range(2):
            first, other = d * half, (1 - d) * half
            owner = (tp + 1 - 2 * d + TP) % TP
            arrived(landing.at[d, k, 0, first : first + half, :], sem.at[d, k, 0])
            piece = table_ref[k, rows(owner * ROWS + first, half), :].astype(jnp.float32)
            piece = piece + landing[d, k, 0, first : first + half, :].astype(jnp.float32)
            passing[d, k, first : first + half, :] = piece.astype(jnp.bfloat16)
            passing[d, k, other : other + half, :] = table_ref[k, rows(owner * ROWS + other, half), :]
            ring_out(d, 1, 0, ROWS, k, passing.at[d, k], group, landing, sem)

    def ring_total(k, table_ref, landing, sem):
        total = table_ref[k, rows(tp * ROWS, ROWS), :].astype(jnp.float32)
        for d in range(2):
            arrived(landing.at[d, k, 1], sem.at[d, k, 1])
            total = total + landing[d, k, 1].astype(jnp.float32)
        return total

    def project(k):
        wo_load(k).wait()
        op_all[k] = jnp.dot(
            attn_s[...], wo[:, cols(k)], preferred_element_type=jnp.float32
        ).astype(jnp.bfloat16)
        ring_first(k, op_all, op_in, 1, op_sem)

    def pass_rows(k, owner, first, count, way):
        ref = zbuf.at[k, rows(owner * ROWS + first, count), :]
        remote(ref, ref, 3, z_sem.at[k, owner], to_z(way)).start()

    def share_rows(k, owner, first, count, way):
        ref = sh_all.at[k, rows(owner * ROWS + first, count), :]
        remote(ref, ref, 2, sh_sem.at[k, owner], to_tp(way)).start()

    def residual(k):
        total = ring_total(k, op_all, op_in, op_sem)
        resid = (stream_s[:, cols(k)].astype(jnp.float32) + total).astype(jnp.bfloat16)
        resid_s[k] = resid
        wide = resid.astype(jnp.float32)
        gain = jnp.concatenate(
            [gain_s[pl.ds(k * (W // 128) + t, 1), :] for t in range(W // 128)], axis=1
        )
        scaled = (wide * gain).astype(jnp.bfloat16)
        zbuf[k, rows(z * ROWS, ROWS), :] = scaled
        sh_all[k, rows(tp * ROWS, ROWS), :] = scaled
        for way in (1, -1):
            pass_rows(k, z, 0, ROWS, way)
            share_rows(k, tp, 0, ROWS, way)
        wide = wide * wide
        square = square_s[...]
        for t in range(W // 128):
            square = square + wide[:, t * 128 : (t + 1) * 128]
        square_s[...] = square

    def send_inverse():
        mean = jnp.sum(square_s[...], axis=1, keepdims=True) * (1.0 / D)
        inverse = jnp.broadcast_to(lax.rsqrt(mean + 1e-06), (ROWS, 128))
        inv_sh[rows(tp * ROWS, ROWS), :] = inverse
        turn_s[rows((z % 2) * ROWS, ROWS), :] = inverse
        inv_own[...] = turn_s[...].T[0:8, :]
        inv_z[z] = inv_own[...]
        for s in range(1, NZ):
            remote(inv_own, inv_z.at[z], 8, inv_z_sem, to_z(s)).start()
        own = inv_sh.at[rows(tp * ROWS, ROWS), :]
        for r in range(1, TP):
            remote(own, own, 9, inv_sh_sem, to_tp(r)).start()

    def spread_inverse():
        arrived(inv_z.at[0 : NZ - 1], inv_z_sem)
        total = jnp.zeros((SLOTS, 128), jnp.float32)
        for q in range(NZ // 2):
            both = inv_z[2 * q] + inv_z[2 * q + 1]
            total = total + place_s[:, q * 128 : (q + 1) * 128].astype(jnp.float32) * both[0:1, :]
        inv_send[...] = jnp.broadcast_to(jnp.sum(total, axis=1, keepdims=True), (SLOTS, 128))
        land = inv_slot.at[rows(mine * GROUP, GROUP), :]
        for s in range(1, SLAB):
            src = inv_send.at[rows(((mine + s) % SLAB) * GROUP, GROUP), :]
            remote(src, land, 10, inv_slot_sem, to_slab(s)).start()
        inv_slot[rows(mine * GROUP, GROUP), :] = inv_send[rows(mine * GROUP, GROUP), :]

    def relay(k, step):
        below, above = (z - step + NZ) % NZ, (z + step) % NZ
        arrived(zbuf.at[k, rows(below * ROWS, ROWS), :], z_sem.at[k, below])
        pass_rows(k, below, 0, ROWS if step < 3 else half, 1)
        arrived(zbuf.at[k, rows(above * ROWS, ROWS), :], z_sem.at[k, above])
        if step < 3:
            pass_rows(k, above, 0, ROWS, -1)
        else:
            pass_rows(k, above, half, half, -1)

    def share(k):
        below, above = (tp + TP - 1) % TP, (tp + 1) % TP
        arrived(sh_all.at[k, rows(below * ROWS, ROWS), :], sh_sem.at[k, below])
        share_rows(k, below, 0, half, 1)
        arrived(sh_all.at[k, rows(above * ROWS, ROWS), :], sh_sem.at[k, above])
        share_rows(k, above, half, half, -1)

    def spread(store, landing, k, sem, group):
        for s in (2, 6, 1, 3, 5, 7, 4):
            src = store.at[k, rows(((mine + s) % SLAB) * GROUP, GROUP), :]
            dst = landing.at[k, rows(mine * GROUP, GROUP), :]
            remote(src, dst, group, sem.at[k], to_slab(s)).start()
        landing[k, rows(mine * GROUP, GROUP), :] = store[k, rows(mine * GROUP, GROUP), :]

    def pack(k):
        far = (z + 4) % NZ
        arrived(zbuf.at[k, rows(far * ROWS, ROWS), :], z_sem.at[k, far])
        ysend[k] = jnp.dot(
            place_s[...], zbuf[k], preferred_element_type=jnp.float32
        ).astype(jnp.bfloat16)
        spread(ysend, xbuf, k, y_sem, 4)

    def enter(k):
        arrived(xbuf.at[k, 0 : SLOTS - GROUP, :], y_sem.at[k])
        hid_s[...] += jnp.dot(xbuf[k], wgu[cols(k), :], preferred_element_type=jnp.float32)

    def gated(sums, inverse):
        g = sums[:, 0:F] * inverse
        return (g / (1.0 + jnp.exp(-g)) * (sums[:, F : 2 * F] * inverse)).astype(jnp.bfloat16)

    def shared():
        def gate(k, acc):
            far = (tp + 2) % TP
            arrived(sh_all.at[k, rows(far * ROWS, ROWS), :], sh_sem.at[k, far])
            return acc + jnp.dot(sh_all[k], sgu[cols(k), :], preferred_element_type=jnp.float32)

        acc = lax.fori_loop(0, NC, gate, jnp.zeros((TP * ROWS, 2 * F), jnp.float32))
        arrived(inv_sh.at[0 : (TP - 1) * ROWS, :], inv_sh_sem)
        hidden = gated(acc, inv_sh[...])

        def down(k, carry):
            sh_out[k] = jnp.dot(
                hidden, sd[:, cols(k)], preferred_element_type=jnp.float32
            ).astype(jnp.bfloat16)
            ring_first(k, sh_out, sh_in, 5, shr_sem)
            return carry

        lax.fori_loop(0, NC, down, 0)

    def guarded(k, action):
        @pl.when((k >= 0) & (k < NC))
        def _():
            action(k)

    def way_out(t, carry):
        guarded(t, project)

        @pl.when(t == RESID_LAG + 2)
        def _():
            for load in loads:
                load.wait()

        guarded(t - SUM_LAG, lambda k: ring_second(k, op_all, op_out, op_in, 1, op_sem))
        for step in (1, 2, 3):
            guarded(t - HOP_LAGS[step - 1], lambda k, step=step: relay(k, step))
        guarded(t - RESID_LAG, residual)

        @pl.when(t == NC - 1 + RESID_LAG)
        def _():
            send_inverse()

        guarded(t - SHARE_LAG, share)
        guarded(t - PACK_LAG, pack)
        guarded(t - ENTER_LAG, enter)

        @pl.when(t == NC + ENTER_LAG - 4)
        def _():
            spread_inverse()

        @pl.when(t == NC + 2 + SHARE_LAG)
        def _():
            shared()

        return carry

    lax.fori_loop(0, NC + ENTER_LAG, way_out, 0)

    arrived(inv_slot.at[0 : SLOTS - GROUP, :], inv_slot_sem)
    hb_s[...] = gated(hid_s[...], inv_slot[...])

    def leave(k):
        rsend[k] = jnp.dot(
            hb_s[...], wd[:, cols(k)], preferred_element_type=jnp.float32
        ).astype(jnp.bfloat16)
        spread(rsend, ret, k, r_sem, 6)

    def hand_on(d, k, stage, first, count):
        src = rs_out.at[d, k, stage, first : first + count, :]
        dst = rs_in.at[d, k, stage, first : first + count, :]
        remote(src, dst, 7, rs_sem.at[d, k, stage], to_z(1 - 2 * d)).start()

    def combine(k):
        arrived(ret.at[k, 0 : SLOTS - GROUP, :], r_sem.at[k])
        part_s[k] = jnp.dot(
            back_hi[...], ret[k], preferred_element_type=jnp.float32
        ) + jnp.dot(back_lo[...], ret[k], preferred_element_type=jnp.float32)
        owner = (z + 4) % NZ
        for d in range(2):
            piece = part_s[k, rows(owner * ROWS + d * half, half), :]
            rs_out[d, k, 0, d * half : (d + 1) * half, :] = piece.astype(jnp.bfloat16)
            hand_on(d, k, 0, d * half, half)

    def add_on(k, stage):
        for d in range(2):
            owner = (z + (1 - 2 * d) * (4 - stage) + NZ) % NZ
            first = d * half if stage == 1 else 0
            count = half if stage == 1 else ROWS
            arrived(rs_in.at[d, k, stage - 1, first : first + count, :], rs_sem.at[d, k, stage - 1])
            piece = part_s[k, rows(owner * ROWS + first, count), :]
            piece = piece + rs_in[d, k, stage - 1, first : first + count, :].astype(jnp.float32)
            rs_out[d, k, stage, first : first + count, :] = piece.astype(jnp.bfloat16)
            if stage == 1:
                other = (1 - d) * half
                piece = part_s[k, rows(owner * ROWS + other, half), :]
                rs_out[d, k, stage, other : other + half, :] = piece.astype(jnp.bfloat16)
            hand_on(d, k, stage, 0, ROWS)

    def finish(k):
        total = part_s[k, rows(z * ROWS, ROWS), :]
        for d in range(2):
            arrived(rs_in.at[d, k, 3], rs_sem.at[d, k, 3])
            total = total + rs_in[d, k, 3].astype(jnp.float32)
        total = total + ring_total(k, sh_out, sh_in, shr_sem)
        out_ref[:, cols(k)] = (resid_s[k].astype(jnp.float32) + total).astype(jnp.bfloat16)

    b1, b2, b3, b4, b5 = RETURN_LAGS

    def give_back(t, carry):
        guarded(t, leave)
        guarded(t - b4, lambda k: add_on(k, 3))
        guarded(t - b3, lambda k: add_on(k, 2))
        guarded(t - b2, lambda k: add_on(k, 1))
        guarded(t - b1, combine)
        guarded(t - b1, lambda k: ring_second(k, sh_out, sh_pass, sh_in, 5, shr_sem))
        guarded(t - b5, finish)
        return carry

    lax.fori_loop(0, NC + b5, give_back, 0)

    left(sh_all.at[:, 0 : 3 * ROWS, :], 1)
    left(sh_all.at[:, 0 : 3 * ROWS, :], 2)
    left(zbuf.at[:, 0 : 7 * ROWS, :], 3)
    left(xbuf.at[:, 0 : SLOTS - GROUP, :], 4)
    left(sh_all.at[:, 0 : 3 * ROWS, :], 5)
    left(ret.at[:, 0 : SLOTS - GROUP, :], 6)
    left(zbuf.at[:, 0 : 7 * ROWS, :], 7)
    left(inv_z.at[0 : NZ - 1], 8)
    left(inv_sh.at[0 : (TP - 1) * ROWS, :], 9)
    left(inv_slot.at[0 : SLOTS - GROUP, :], 10)


def moe(
    attn_rows, stream_in, norm_gain, places, w_out, w_gate, w_up, w_down, s_gate, s_up, s_down
):
    vmem = pl.BlockSpec(memory_space=pltpu.VMEM)
    hbm = pl.BlockSpec(memory_space=pl.ANY)
    bf, f32 = jnp.bfloat16, jnp.float32
    dma = pltpu.SemaphoreType.DMA
    return pl.pallas_call(
        moe_kernel,
        out_shape=jax.ShapeDtypeStruct((ROWS, D), bf),
        in_specs=[hbm] * 13,
        out_specs=vmem,
        scratch_shapes=[
            pltpu.VMEM((TP * ROWS, 2 * VD), bf),
            pltpu.VMEM((ROWS, D), bf),
            pltpu.VMEM((D // 128, 128), f32),
            pltpu.VMEM((2 * VD, D), bf),
            pltpu.VMEM((D, 2 * F), bf),
            pltpu.VMEM((F, D), bf),
            pltpu.VMEM((D, 2 * F), bf),
            pltpu.VMEM((F, D), bf),
            pltpu.VMEM((NC, TP * ROWS, W), bf),
            pltpu.VMEM((2, NC, ROWS, W), bf),
            pltpu.VMEM((2, NC, 2, ROWS, W), bf),
            pltpu.VMEM((NC, ROWS, W), bf),
            pltpu.VMEM((ROWS, 128), f32),
            pltpu.VMEM((NC, NZ * ROWS, W), bf),
            pltpu.VMEM((SLOTS, NZ * ROWS), bf),
            pltpu.VMEM((NZ * ROWS, SLOTS), bf),
            pltpu.VMEM((NZ * ROWS, SLOTS), bf),
            pltpu.VMEM((2 * ROWS, 128), f32),
            pltpu.VMEM((8, 128), f32),
            pltpu.VMEM((NZ, 8, 128), f32),
            pltpu.VMEM((SLOTS, 128), f32),
            pltpu.VMEM((SLOTS, 128), f32),
            pltpu.VMEM((TP * ROWS, 128), f32),
            pltpu.VMEM((NC, SLOTS, W), bf),
            pltpu.VMEM((NC, SLOTS, W), bf),
            pltpu.VMEM((SLOTS, 2 * F), f32),
            pltpu.VMEM((SLOTS, F), bf),
            pltpu.VMEM((NC, SLOTS, W), bf),
            pltpu.VMEM((NC, SLOTS, W), bf),
            pltpu.VMEM((NC, NZ * ROWS, W), f32),
            pltpu.VMEM((2, NC, 4, ROWS, W), bf),
            pltpu.VMEM((2, NC, 4, ROWS, W), bf),
            pltpu.VMEM((NC, TP * ROWS, W), bf),
            pltpu.VMEM((NC, TP * ROWS, W), bf),
            pltpu.VMEM((2, NC, ROWS, W), bf),
            pltpu.VMEM((2, NC, 2, ROWS, W), bf),
            dma((NC,)),
            dma((12,)),
            dma((11,)),
            dma((2, NC, 2)),
            dma((NC, NZ)),
            dma((NC,)),
            dma((NC,)),
            dma((2, NC, 4)),
            dma((NC, TP)),
            dma((2, NC, 2)),
            dma,
            dma,
            dma,
        ],
        compiler_params=pltpu.CompilerParams(
            collective_id=1, has_side_effects=True, vmem_limit_bytes=67043328
        ),
        name="experts",
    )(
        attn_rows, stream_in, norm_gain.reshape(D // 128, 128), *places,
        w_out, w_gate, w_up, w_down, s_gate, s_up, s_down,
    )


def local(
    stream_in,
    q_first,
    q_second,
    k_first,
    k_second,
    values,
    head_lambda,
    w_out,
    norm_gain,
    routes,
    route_w,
    w_gate,
    w_up,
    w_down,
    s_gate,
    s_up,
    s_down,
):
    attn_rows, *places = attention(
        head_lambda, q_first, q_second, k_first, k_second, values, routes, route_w
    )
    return moe(
        attn_rows, stream_in, norm_gain, places, w_out, w_gate, w_up, w_down, s_gate, s_up, s_down
    )


def solution(mesh):
    return jax.shard_map(
        local,
        mesh=mesh,
        in_specs=(
            P(("sp", "tp"), None),
            P("sp", "tp"),
            P("sp", "tp"),
            P("sp", "tp"),
            P("sp", "tp"),
            P("sp", "tp"),
            P("tp"),
            P("tp", None),
            P(),
            P(("sp", "tp"), None),
            P(("sp", "tp"), None),
            P("sp", None, None),
            P("sp", None, None),
            P("sp", None, None),
            P(None, "tp"),
            P(None, "tp"),
            P("tp", None),
        ),
        out_specs=P(("sp", "tp"), None),
        check_vma=False,
    )
```
